32 devices in a mesh: rep: 2 (over y), fs: 4 (over z), tp: 4 (over x, core).
Axes of the slice: x: 2, y: 2, z: 4, core: 2. Of those that a mesh axis runs over, the one named last changes fastest.
Arguments:
- tokens: bfloat16 [4096, 2048], P(('rep', 'fs'), 'tp'), may hold values from -6 to 6
- pre_gain: float32 [2048], replicated, may hold values from 0.1 to 1.9
- u_weight: float32 [2048, 512], P('fs', 'tp'), may hold values from -0.125 to 0.125
- u_scale: float32 [512], P('tp'), may hold values from 0.5 to 2
- v_weight: float32 [2048, 512], P('fs', 'tp'), may hold values from -0.125 to 0.125
- v_scale: float32 [512], P('tp'), may hold values from 0.5 to 2
- group_gain: float32 [512], P('tp'), may hold values from 0.1 to 1.9
- span_weight: bfloat16 [8, 128, 128], P('tp'), may hold values from -0.5 to 0.5
- span_bias: float32 [8, 128], P('tp'), may hold values from 0.5 to 1.5
- out_weight: float32 [512, 2048], P('tp', 'fs'), may hold values from -0.25 to 0.25
- out_scale: float32 [2048], P('fs'), may hold values from 0.5 to 2
- ffn_gain: float32 [2048], replicated, may hold values from 0.1 to 1.9
- gate_weight: float32 [2048, 5632], P('fs', 'tp'), may hold values from -0.125 to 0.125
- gate_scale: float32 [5632], P('tp'), may hold values from 0.5 to 2
- up_weight: float32 [2048, 5632], P('fs', 'tp'), may hold values from -0.125 to 0.125
- up_scale: float32 [5632], P('tp'), may hold values from 0.5 to 2
- down_weight: float32 [5632, 2048], P('tp', 'fs'), may hold values from -0.078125 to 0.078125
- down_scale: float32 [2048], P('fs'), may hold values from 0.5 to 2
Outputs:
- layer_out: bfloat16 [4096, 2048], P(('rep', 'fs'), 'tp')
The draws below stay inside these ranges and needn't reach their ends.
All inputs are finite; a program needn't handle non-finite values.
Results may differ from the reference program's by a relative error of at most 0.02.
Values may be sent and summed in bfloat16 or wider, within the bound.
A program may use at most 64 MiB of HBM per device.

```python
import math
import jax
import jax.numpy as jnp
from jax import lax

D = 2048
GROUPS = 8
GROUP_DIM = 64
MIX_WIDTH = 512
HIDDEN_SIZE = 5632
SPAN = 128
TOKENS = 4096
N_TP = 4


def levels(rng, shape, shards, smallest, largest):
    def one(dim, shards_of):
        steps = jax.random.uniform(jax.random.fold_in(jax.random.fold_in(rng, 6), dim), (shards_of,), jnp.float32, smallest / len(shards), largest / len(shards))
        return jnp.repeat(jnp.exp(steps), shape[dim] // shards_of).reshape((-1,) + (1,) * (len(shape) - dim - 1))

    level = one(*shards[0])
    for cut in shards[1:]:
        level = level * one(*cut)
    return level


def normal_values(key, extent, scale, reach, shards=(), held_as=jnp.bfloat16):
    entries = jax.random.normal(key, extent, jnp.float32) * scale
    if len(shards) > 0:
        entries = levels(key, extent, shards, -0.22, 0.18) * entries
    return jnp.clip(entries, min=-reach, max=reach).astype(held_as)


def setup_inputs(seed: int = 0) -> dict:
    arg_keys = jax.random.split(jax.random.key(seed), 19)
    tokens = normal_values(arg_keys[0], (TOKENS, D), 1.0, 6.0, ((0, 8), (1, 4)))
    pre_gain = jnp.clip(1.0 + 0.18 * jax.random.normal(arg_keys[1], (D,), jnp.float32), 0.1, 1.9)
    u_weight = normal_values(arg_keys[2], (D, MIX_WIDTH), D ** -0.5, 0.125, ((0, 4), (1, 4)), jnp.float32)
    u_scale = jnp.clip(jnp.exp(math.log(2.0) - 1.3862944 * jax.random.uniform(arg_keys[3], (MIX_WIDTH,), jnp.float32) ** levels(arg_keys[3], (MIX_WIDTH,), ((0, 4),), -0.2, 0.2)), 0.5, 2.0)
    v_weight = normal_values(arg_keys[4], (D, MIX_WIDTH), D ** -0.5, 0.125, ((0, 4), (1, 4)), jnp.float32)
    v_scale = jnp.clip(jnp.exp(math.log(2.0) - 1.3862944 * jax.random.uniform(arg_keys[5], (MIX_WIDTH,), jnp.float32) ** levels(arg_keys[5], (MIX_WIDTH,), ((0, 4),), -0.2, 0.2)), 0.5, 2.0)
    group_gain = jnp.clip(1.0 + 0.18 * jax.random.normal(arg_keys[6], (MIX_WIDTH,), jnp.float32), 0.1, 1.9)
    span_weight = normal_values(arg_keys[7], (GROUPS, SPAN, SPAN), SPAN ** -0.5, 0.5, ((0, 4),))
    span_bias = jnp.clip(0.5 + 1.0 * jax.random.uniform(arg_keys[8], (GROUPS, SPAN), jnp.float32) ** levels(arg_keys[8], (GROUPS, SPAN), ((0, 4),), -0.2, 0.2), 0.5, 1.5)
    out_weight = normal_values(arg_keys[9], (MIX_WIDTH, D), MIX_WIDTH ** -0.5, 0.25, ((0, 4), (1, 4)), jnp.float32)
    out_scale = jnp.clip(jnp.exp(math.log(2.0) - 1.3862944 * jax.random.uniform(arg_keys[10], (D,), jnp.float32) ** levels(arg_keys[10], (D,), ((0, 4),), -0.2, 0.2)), 0.5, 2.0)
    ffn_gain = jnp.clip(1.0 + 0.18 * jax.random.normal(arg_keys[11], (D,), jnp.float32), 0.1, 1.9)
    gate_weight = normal_values(arg_keys[12], (D, HIDDEN_SIZE), D ** -0.5, 0.125, ((0, 4), (1, 4)), jnp.float32)
    gate_scale = jnp.clip(jnp.exp(math.log(2.0) - 1.3862944 * jax.random.uniform(arg_keys[13], (HIDDEN_SIZE,), jnp.float32) ** levels(arg_keys[13], (HIDDEN_SIZE,), ((0, 4),), -0.2, 0.2)), 0.5, 2.0)
    up_weight = normal_values(arg_keys[14], (D, HIDDEN_SIZE), D ** -0.5, 0.125, ((0, 4), (1, 4)), jnp.float32)
    up_scale = jnp.clip(jnp.exp(math.log(2.0) - 1.3862944 * jax.random.uniform(arg_keys[15], (HIDDEN_SIZE,), jnp.float32) ** levels(arg_keys[15], (HIDDEN_SIZE,), ((0, 4),), -0.2, 0.2)), 0.5, 2.0)
    down_weight = normal_values(arg_keys[16], (HIDDEN_SIZE, D), HIDDEN_SIZE ** -0.5, 0.078125, ((0, 4), (1, 4)), jnp.float32)
    down_scale = jnp.clip(jnp.exp(math.log(2.0) - 1.3862944 * jax.random.uniform(arg_keys[17], (D,), jnp.float32) ** levels(arg_keys[17], (D,), ((0, 4),), -0.2, 0.2)), 0.5, 2.0)
    return {"tokens": tokens, "pre_gain": pre_gain, "u_weight": u_weight, "u_scale": u_scale, "v_weight": v_weight, "v_scale": v_scale, "group_gain": group_gain, "span_weight": span_weight, "span_bias": span_bias, "out_weight": out_weight, "out_scale": out_scale, "ffn_gain": ffn_gain, "gate_weight": gate_weight, "gate_scale": gate_scale, "up_weight": up_weight, "up_scale": up_scale, "down_weight": down_weight, "down_scale": down_scale}


EPS = 0.02

def rms_rows(values, gain):
    wide = values.astype(jnp.float32)
    scaled = wide * lax.rsqrt(lax.optimization_barrier(jnp.mean(wide * wide, axis=-1, keepdims=True)) + EPS)
    return (scaled * gain).astype(jnp.bfloat16)

def block_sum(acts, weight, scale):
    width = acts.shape[1] // N_TP
    acts_blocks = jnp.moveaxis(acts.reshape(acts.shape[0], N_TP, width), 1, 0)
    weight_blocks = weight.astype(jnp.bfloat16).reshape(N_TP, width, weight.shape[1])

    def add_block(total, pair):
        term = (jnp.dot(pair[0], pair[1], preferred_element_type=jnp.float32) * scale).astype(jnp.bfloat16)
        return (total + term.astype(jnp.float32), None)
    start = jnp.zeros((acts.shape[0], weight.shape[1]), jnp.float32)
    total, unused = lax.scan(add_block, start, (acts_blocks, weight_blocks))
    return total.astype(jnp.bfloat16)

def reference(tokens, pre_gain, u_weight, u_scale, v_weight, v_scale, group_gain, span_weight, span_bias, out_weight, out_scale, ffn_gain, gate_weight, gate_scale, up_weight, up_scale, down_weight, down_scale):
    row_count = tokens.shape[0]
    normed = rms_rows(tokens, pre_gain)
    u_act = jax.nn.gelu(jnp.dot(normed, u_weight.astype(jnp.bfloat16), preferred_element_type=jnp.float32) * u_scale)
    v_act = jax.nn.gelu(jnp.dot(normed, v_weight.astype(jnp.bfloat16), preferred_element_type=jnp.float32) * v_scale)
    grouped = v_act.reshape(row_count, GROUPS, GROUP_DIM)
    centre = lax.optimization_barrier(jnp.mean(grouped, axis=-1, keepdims=True))
    spread = lax.optimization_barrier(jnp.mean(jnp.square(grouped - centre), axis=-1, keepdims=True))
    v_norm = (((grouped - centre) * lax.rsqrt(spread + EPS)).reshape(row_count, MIX_WIDTH) * group_gain).astype(jnp.bfloat16)
    spans = v_norm.reshape(row_count // SPAN, SPAN, GROUPS, GROUP_DIM).astype(jnp.float32)
    lower = jnp.tril(span_weight).astype(jnp.float32)
    mixed = jnp.einsum('gts,nsgc->ntgc', lower, spans) + jnp.transpose(span_bias)[None, :, :, None]
    gated = (u_act * mixed.reshape(row_count, MIX_WIDTH)).astype(jnp.bfloat16)
    mix = (jnp.dot(gated, out_weight.astype(jnp.bfloat16), preferred_element_type=jnp.float32) * out_scale).astype(jnp.bfloat16)
    resid = (tokens.astype(jnp.float32) + mix.astype(jnp.float32)).astype(jnp.bfloat16)
    normed_ffn = rms_rows(resid, ffn_gain)
    gate_pre = jnp.dot(normed_ffn, gate_weight.astype(jnp.bfloat16), preferred_element_type=jnp.float32) * gate_scale
    up_pre = jnp.dot(normed_ffn, up_weight.astype(jnp.bfloat16), preferred_element_type=jnp.float32) * up_scale
    hidden = (jax.nn.silu(gate_pre) * up_pre).astype(jnp.bfloat16)
    ffn = block_sum(hidden, down_weight, down_scale)
    return (resid.astype(jnp.float32) + ffn.astype(jnp.float32)).astype(jnp.bfloat16)
```

```python
import functools

import jax
import jax.numpy as jnp
from jax import lax
from jax.experimental import pallas as pl
from jax.experimental.pallas import tpu as pltpu
from jax.sharding import PartitionSpec as P

EPS = 0.02
MESH = pl.DeviceIdType.MESH
LANES = 128
UV, GU0, GU1, DN0, DN1 = range(5)
KINDS = 5
TOK, GATED, OWN, PAIR = range(4)
CHUNK = 256


def on(condition, action):
    if isinstance(condition, bool):
        if condition:
            action()
    else:
        pl.when(condition)(action)


def flip(a, d, size):
    total, bit = 0, 1
    while bit < size:
        total = total + lax.rem(lax.div(a, jnp.int32(bit)) + lax.div(jnp.int32(d), jnp.int32(bit)), jnp.int32(2)) * bit
        bit *= 2
    return total


def loop(low, high, body):
    def step(i, carry):
        body(i)
        return carry

    lax.fori_loop(low, high, step, 0)


def layer_kernel(
    sizes,
    tokens_ref,
    u_ref,
    v_ref,
    out_ref,
    gate_ref,
    up_ref,
    down_ref,
    out_scale_ref,
    down_scale_ref,
    pre_gain_ref,
    ffn_gain_ref,
    u_scale_ref,
    v_scale_ref,
    group_gain_ref,
    span_ref,
    bias_ref,
    gate_scale_ref,
    up_scale_ref,
    result_ref,
    u_f,
    v_f,
    out_f,
    gate_f,
    up_f,
    down_f,
    out_own,
    gu_own,
    down_own,
    tok_all,
    uv_all,
    out_all,
    scale_all,
    gated_all,
    resid_all,
    normed,
    gu_all,
    down_all,
    gu_acc,
    hidden,
    part,
    mate_in,
    x_in,
    pair_in,
    local_sem,
    z_send,
    z_recv,
    y_send,
    y_recv,
    e_send,
    e_recv,
    p_send,
    p_recv,
    o_send,
    o_recv,
    s_send,
    s_recv,
    m_send,
    m_recv,
    x_send,
    x_recv,
    q_send,
    q_recv,
):
    n_rep, n_fs, n_tp = sizes
    n_x = n_tp // 2
    rows, own_width = tokens_ref.shape
    block = gate_ref.shape[0]
    per_own = own_width // block
    hid = gate_ref.shape[1] // 2
    main = hid // LANES * LANES
    channels = u_ref.shape[1]
    groups, span = span_ref.shape[0], span_ref.shape[1]
    spans = rows // span
    total_rows = 2 * rows
    chunks = total_rows // CHUNK
    half_chunks = chunks // 2
    rep, fs, tp = lax.axis_index("rep"), lax.axis_index("fs"), lax.axis_index("tp")
    two = jnp.int32(2)
    member = lax.rem(fs, two)
    core, xi = lax.rem(tp, two), lax.div(tp, two)
    mate = tp + 1 - 2 * core
    pair = fs + 1 - 2 * member
    owner = lax.div(fs, jnp.int32(per_own))
    owner_sub = lax.rem(fs, jnp.int32(per_own))

    def copy(src, dst, send_sem, recv_sem, **device):
        return pltpu.make_async_remote_copy(
            src_ref=src, dst_ref=dst, send_sem=send_sem, recv_sem=recv_sem, device_id=device, device_id_type=MESH)

    def rows_at(i, size):
        return pl.ds(pl.multiple_of(i * size, size), size)

    k_uv, k_gu, k_dn = block // n_rep, block // n_rep // 2, hid // n_rep // 2

    def w_rows(kind, r):
        if kind == UV:
            return pl.ds(pl.multiple_of(r * k_uv, k_uv), k_uv)
        if kind in (GU0, GU1):
            return pl.ds(pl.multiple_of((2 * r + (kind - GU0)) * k_gu, k_gu), k_gu)
        return pl.ds(pl.multiple_of((2 * r + (kind - DN0)) * k_dn, k_dn), k_dn)

    def w_slot(kind, f, r):
        ref = uv_all if kind == UV else gu_all if kind in (GU0, GU1) else down_all
        return ref.at[f, w_rows(kind, r)]

    def w_source(kind, g):
        if kind == UV:
            return w_slot(UV, fs, rep)
        ref = gu_own if kind in (GU0, GU1) else down_own
        return ref.at[lax.rem(g, two), w_rows(kind, rep)]

    def z_copy(kind, d):
        g = flip(fs, d, n_fs)
        return copy(w_source(kind, g), w_slot(kind, fs, rep), z_send.at[kind, d - 1], z_recv.at[kind, d - 1], fs=g)

    def y_copy(kind, d, e):
        slot = w_slot(kind, flip(fs, d, n_fs), rep)
        return copy(slot, slot, y_send.at[kind, d - 1, e - 1], y_recv.at[kind, d - 1, e - 1],
                    rep=lax.rem(rep + e, jnp.int32(n_rep)))

    def z_start(kind):
        loop(1, n_fs, lambda d: z_copy(kind, d).start())

    def y_relay(kind, d):
        slot = w_slot(kind, flip(fs, d, n_fs), rep)
        copy(slot, slot, z_send.at[kind, d - 1], z_recv.at[kind, d - 1], fs=pair).wait_recv()
        for e in range(1, n_rep):
            y_copy(kind, d, e).start()

    def y_ready(kind, d):
        for e in range(1, n_rep):
            slot = w_slot(kind, flip(fs, d, n_fs), lax.rem(rep - e + n_rep, jnp.int32(n_rep)))
            copy(slot, slot, y_send.at[kind, d - 1, e - 1], y_recv.at[kind, d - 1, e - 1],
                 rep=lax.rem(rep + 1, jnp.int32(n_rep))).wait_recv()

    def e_slot(kind, i, t):
        here = rows_at(i, span)
        if kind == TOK:
            return tok_all.at[t, here]
        if kind == GATED:
            return gated_all.at[t, here]
        return resid_all.at[member if kind == OWN else 1 - member, t, here]

    def x_peer(dx):
        return 2 * flip(xi, dx, n_x) + core

    def e_copy(kind, i, t, k, to):
        slot = e_slot(kind, i, t)
        return copy(slot, slot, e_send.at[kind, i, k], e_recv.at[kind, i, t], tp=to)

    def e_list(kind, i):
        out = [e_copy(kind, i, tp, 0, mate)]
        for dx in range(1, n_x):
            out.append(e_copy(kind, i, tp, dx, x_peer(dx)))
        return out

    def e_push(kind, i):
        for c in e_list(kind, i):
            c.start()

    def e_wait(kind, i, t):
        e_copy(kind, i, t, 0, mate).wait_recv()

    def e_relay(kind, i):
        for dx in range(1, n_x):
            e_wait(kind, i, x_peer(dx))
            e_copy(kind, i, x_peer(dx), n_x - 1 + dx, mate).start()

    def e_finish(kind, i):
        for dx in range(n_x):
            e_wait(kind, i, 2 * flip(xi, dx, n_x) + 1 - core)

    def e_sent(kind, i):
        for c in e_list(kind, i):
            c.wait_send()
        for dx in range(1, n_x):
            e_copy(kind, i, x_peer(dx), n_x - 1 + dx, mate).wait_send()

    def p_copy(i, which):
        slot = resid_all.at[which, tp, rows_at(i, span)]
        return copy(slot, slot, p_send.at[i], p_recv.at[i], fs=pair)

    def o_copy(d):
        g = flip(fs, d, n_fs)
        return copy(out_own, out_all.at[tp, owner_sub], o_send.at[d], o_recv.at[tp, owner_sub], fs=g, tp=owner)

    def o_each(action):
        def body(d):
            on(jnp.logical_or(d > 0, owner != tp), lambda: action(d))

        loop(0, n_fs, body)

    def s_copy(d, which):
        g = flip(fs, d, n_fs)
        src = (out_scale_ref, down_scale_ref)[which]
        return copy(src, scale_all.at[which, owner_sub], s_send.at[which, d - 1], s_recv.at[which, owner_sub], fs=g)

    loads = [
        pltpu.make_async_copy(src, dst, local_sem.at[i])
        for i, (src, dst) in enumerate((
            (tokens_ref, tok_all.at[tp]), (u_ref, u_f), (v_ref, v_f), (out_ref, out_f), (gate_ref, gate_f),
            (up_ref, up_f), (down_ref, down_f)))
    ]
    for load in loads:
        load.start()

    barrier = pltpu.get_barrier_semaphore()

    def greet(**device):
        pl.semaphore_signal(barrier, inc=1, device_id=device, device_id_type=MESH)

    greet(tp=mate)
    for dx in range(1, n_x):
        greet(tp=x_peer(dx))
    loop(1, n_fs, lambda d: greet(fs=flip(fs, d, n_fs)))
    for e in range(1, n_rep):
        greet(rep=lax.rem(rep + e, jnp.int32(n_rep)))

    def greet_source(i):
        f, t = tp * per_own + lax.div(i, jnp.int32(n_tp)), lax.rem(i, jnp.int32(n_tp))
        on(jnp.logical_or(f != fs, t != tp), lambda: greet(fs=f, tp=t))

    loop(0, per_own * n_tp, greet_source)
    pl.semaphore_wait(barrier, 1 + (n_x - 1) + (n_fs - 1) + (n_rep - 1) + jnp.where(owner == tp, n_fs - 1, n_fs))

    loads[0].wait()
    loop(0, spans, lambda i: e_push(TOK, i))
    loads[1].wait()
    loads[2].wait()
    uv_all[fs, :, 0:channels] = u_f[...].astype(jnp.bfloat16)
    uv_all[fs, :, channels:2 * channels] = v_f[...].astype(jnp.bfloat16)
    z_start(UV)
    loads[3].wait()
    out_own[...] = out_f[...].astype(jnp.bfloat16)

    def keep_own():
        out_all[tp, owner_sub] = out_f[...].astype(jnp.bfloat16)
        scale_all[0, owner_sub] = out_scale_ref[...]
        scale_all[1, owner_sub] = down_scale_ref[...]

    on(owner == tp, keep_own)
    o_each(lambda d: o_copy(d).start())

    def s_each(action):
        def body(d):
            for which in range(2):
                action(s_copy(d, which))

        on(owner == tp, lambda: loop(1, n_fs, body))

    s_each(lambda c: c.start())

    low = lax.broadcasted_iota(jnp.int32, (1, LANES), 1) < LANES // 2
    unit = 64

    def swap(value):
        return pltpu.roll(value, LANES // 2, 1)

    loads[4].wait()
    loads[5].wait()

    def cast_gu(i):
        here = rows_at(i, unit)
        for member_of in range(2):
            first = member_of * (main + LANES)
            gu_own[member_of, here, 0:main] = gate_f[here, first:first + main].astype(jnp.bfloat16)
            gu_own[member_of, here, main:2 * main] = up_f[here, first:first + main].astype(jnp.bfloat16)
        g, u = gate_f[here, main:main + LANES], up_f[here, main:main + LANES]
        gu_own[0, here, 2 * main:] = jnp.where(low, g, swap(u)).astype(jnp.bfloat16)
        gu_own[1, here, 2 * main:] = jnp.where(low, swap(g), u).astype(jnp.bfloat16)

    loop(0, block // unit, cast_gu)
    z_start(GU0)
    keep_gu = pltpu.make_async_copy(gu_own.at[member], gu_all.at[fs], local_sem.at[7])
    keep_gu.start()
    loads[6].wait()

    def cast_down(i):
        here = rows_at(i, unit)
        down_own[0, here] = down_f[here].astype(jnp.bfloat16)
        there = jnp.where(i < main // unit, i + (main + LANES) // unit, main // unit + 1)
        down_own[1, here] = down_f[rows_at(there, unit)].astype(jnp.bfloat16)

    loop(0, hid // unit, cast_down)
    keep_down = pltpu.make_async_copy(down_own.at[member], down_all.at[fs], local_sem.at[8])
    keep_down.start()

    loop(0, spans, lambda i: e_relay(TOK, i))
    loop(1, n_fs, lambda d: y_relay(UV, d))
    loop(1, n_fs, lambda d: y_ready(UV, d))

    eye = lax.broadcasted_iota(jnp.int32, (span, span), 0) == lax.broadcasted_iota(jnp.int32, (span, span), 1)
    tril = lax.broadcasted_iota(jnp.int32, (span, span), 0) >= lax.broadcasted_iota(jnp.int32, (span, span), 1)

    def mixer_span(i):
        e_finish(TOK, i)
        here = rows_at(i, span)
        square = jnp.zeros((span, 1), jnp.float32)
        for t in range(n_tp):
            wide = tok_all[t, here, :].astype(jnp.float32)
            square += jnp.sum(wide * wide, axis=-1, keepdims=True)
        inverse = lax.rsqrt(square / (n_tp * own_width) + EPS)
        pre = None
        for f in range(n_fs):
            t, sub = f // per_own, f % per_own
            wide = tok_all[t, here, sub * block:(sub + 1) * block].astype(jnp.float32)
            source = (wide * inverse * pre_gain_ref[:, f * block:(f + 1) * block]).astype(jnp.bfloat16)
            term = jnp.dot(source, uv_all[f], preferred_element_type=jnp.float32)
            pre = term if f == 0 else pre + term
        u_act = jax.nn.gelu(pre[:, :channels] * u_scale_ref[...])
        v_act = jax.nn.gelu(pre[:, channels:] * v_scale_ref[...])
        width = channels // groups
        group_of = lax.broadcasted_iota(jnp.int32, v_act.shape, 1) // width
        centre = jnp.zeros_like(v_act)
        for g in range(groups):
            mean = jnp.sum(jnp.where(group_of == g, v_act, 0.0), axis=-1, keepdims=True) / width
            centre = jnp.where(group_of == g, mean, centre)
        apart = v_act - centre
        square = apart * apart
        inverse = jnp.zeros_like(v_act)
        for g in range(groups):
            spread = jnp.sum(jnp.where(group_of == g, square, 0.0), axis=-1, keepdims=True) / width
            inverse = jnp.where(group_of == g, lax.rsqrt(spread + EPS), inverse)
        v_norm = (apart * inverse * group_gain_ref[...]).astype(jnp.bfloat16)
        mixed = jnp.zeros_like(v_act)
        for g in range(groups):
            lower = jnp.where(tril, span_ref[g].astype(jnp.float32), 0.0).astype(jnp.bfloat16)
            bias = jnp.sum(jnp.where(eye, bias_ref[g:g + 1, :], 0.0), axis=1, keepdims=True)
            term = jnp.dot(lower, v_norm, preferred_element_type=jnp.float32) + bias
            mixed = jnp.where(group_of == g, term, mixed)
        gated_all[tp, here, :] = (u_act * mixed).astype(jnp.bfloat16)
        e_push(GATED, i)

    loop(0, spans, mixer_span)
    loop(0, spans, lambda i: e_relay(GATED, i))

    def out_arrived(i):
        sub, t = lax.div(i, jnp.int32(n_tp)), lax.rem(i, jnp.int32(n_tp))
        on(jnp.logical_or(tp * per_own + sub != fs, t != tp),
           lambda: copy(out_own, out_all.at[t, sub], o_send.at[0], o_recv.at[t, sub], fs=pair, tp=mate).wait_recv())

    loop(0, per_own * n_tp, out_arrived)

    def scale_arrived(sub):
        def take():
            for which in range(2):
                copy(out_scale_ref, scale_all.at[which, sub], s_send.at[which, 0], s_recv.at[which, sub],
                     fs=pair).wait_recv()

        on(tp * per_own + sub != fs, take)

    loop(0, per_own, scale_arrived)

    def resid_span(i):
        e_finish(GATED, i)
        here = rows_at(i, span)
        for sub in range(per_own):
            mix = None
            for s in range(n_tp):
                term = jnp.dot(gated_all[s, here, :], out_all[s, sub], preferred_element_type=jnp.float32)
                mix = term if s == 0 else mix + term
            mix = (mix * scale_all[0, sub]).astype(jnp.bfloat16)
            cols = slice(sub * block, (sub + 1) * block)
            resid_all[member, tp, here, cols] = (
                tok_all[tp, here, cols].astype(jnp.float32) + mix.astype(jnp.float32)).astype(jnp.bfloat16)
        e_push(OWN, i)
        p_copy(i, member).start()

    loop(0, spans, resid_span)
    for kind in (GU1, DN0, DN1):
        z_start(kind)

    def norm_span(which, i):
        here = rows_at(i, span)
        square = jnp.zeros((span, 1), jnp.float32)
        for t in range(n_tp):
            wide = resid_all[which, t, here, :].astype(jnp.float32)
            square += jnp.sum(wide * wide, axis=-1, keepdims=True)
        inverse = lax.rsqrt(square / (n_tp * own_width) + EPS)
        there = rows_at(which * spans + i, span)
        for f in range(n_fs):
            t, sub = f // per_own, f % per_own
            wide = resid_all[which, t, here, sub * block:(sub + 1) * block].astype(jnp.float32)
            gain = ffn_gain_ref[:, f * block:(f + 1) * block]
            normed[f, there, :] = (wide * inverse * gain).astype(jnp.bfloat16)

    loop(0, spans, lambda i: e_relay(OWN, i))

    def own_span(i):
        e_finish(OWN, i)
        norm_span(member, i)

    loop(0, spans, own_span)
    loop(1, n_fs, lambda d: y_relay(GU0, d))

    def pair_span(i):
        p_copy(i, 1 - member).wait_recv()
        e_push(PAIR, i)

    loop(0, spans, pair_span)
    loop(0, spans, lambda i: e_relay(PAIR, i))

    def other_span(i):
        e_finish(PAIR, i)
        norm_span(1 - member, i)

    loop(0, spans, other_span)

    keep_gu.wait()

    def first_gu(i):
        here = rows_at(i, CHUNK)
        gu_acc[here, :] = jnp.dot(normed[fs, here, :], gu_all[fs], preferred_element_type=jnp.float32)

    loop(0, chunks, first_gu)
    loop(1, n_fs, lambda d: y_relay(GU1, d))

    def fold_gu(d):
        y_ready(GU0, d)
        y_ready(GU1, d)
        f = flip(fs, d, n_fs)

        def body(i):
            here = rows_at(i, CHUNK)
            gu_acc[here, :] += jnp.dot(normed[f, here, :], gu_all[f], preferred_element_type=jnp.float32)

        loop(0, chunks, body)

    loop(1, n_fs, fold_gu)

    second = member == 1

    def main_scale(ref):
        return jnp.where(second, ref[:, main + LANES:], ref[:, 0:main])

    gate_main, up_main = main_scale(gate_scale_ref), main_scale(up_scale_ref)
    gs, us = gate_scale_ref[:, main:main + LANES], up_scale_ref[:, main:main + LANES]
    last_scale = jnp.where(second, jnp.where(low, swap(gs), us), jnp.where(low, gs, swap(us)))

    def hidden_chunk(i):
        here = rows_at(i, 64)
        a = gu_acc[here, 0:main] * gate_main
        b = gu_acc[here, main:2 * main] * up_main
        hidden[here, 0:main] = (a / (1.0 + jnp.exp(-a)) * b).astype(jnp.bfloat16)
        a = gu_acc[here, 2 * main:] * last_scale
        b = swap(a)
        last = (a / (1.0 + jnp.exp(-a)) * b).astype(jnp.bfloat16)
        hidden[here, main:hid] = last[:, 0:hid - main]

    loop(0, total_rows // 64, hidden_chunk)
    keep_down.wait()

    def block_at(k):
        return fs - member + 0 if k is None else flip(fs - member, k, n_fs)

    def places(k):
        b = block_at(k)
        own = lax.div(b, jnp.int32(per_own))
        return b, lax.rem(own, two), lax.div(own, two), lax.rem(b, jnp.int32(per_own)), own

    def m_copy(k, j):
        b, oc, ox, sub, own = places(k)
        here = rows_at(j, CHUNK)
        return copy(part.at[b, here], mate_in.at[ox, sub, here], m_send.at[b, j], m_recv.at[ox, sub, j], tp=mate)

    def x_copy(k, j):
        b, oc, ox, sub, own = places(k)
        here = rows_at(j, CHUNK)
        d = flip(xi, ox, n_x)
        return copy(part.at[b, here], x_in.at[d - 1, sub, here], x_send.at[b, j], x_recv.at[d - 1, sub, j], tp=own)

    def q_copy(k, j):
        b, oc, ox, sub, own = places(k)
        src = part.at[b, rows_at((1 - member) * half_chunks + j, CHUNK)]
        return copy(src, pair_in.at[sub, rows_at(j, CHUNK)], q_send.at[sub, j], q_recv.at[sub, j], fs=pair)

    def down_one(k):
        b, oc, ox, sub, own = places(k)
        d = flip(member, k, n_fs)

        def ready():
            y_ready(DN0, d)
            y_ready(DN1, d)

        on(d > 0, ready)

        def body(j):
            here = rows_at(j, CHUNK)
            part[b, here, :] = jnp.dot(hidden[here, :], down_all[b], preferred_element_type=jnp.float32).astype(
                jnp.bfloat16)
            on(core != oc, lambda: m_copy(k, j).start())

        loop(0, chunks, body)

    def across(k):
        b, oc, ox, sub, own = places(k)

        def body(j):
            here = rows_at(j, CHUNK)
            m_copy(k, j).wait_recv()
            part[b, here, :] = (part[b, here, :].astype(jnp.float32)
                                + mate_in[ox, sub, here, :].astype(jnp.float32)).astype(jnp.bfloat16)
            on(xi != ox, lambda: x_copy(k, j).start())

        on(core == oc, lambda: loop(0, chunks, body))

    def collect(k):
        b, oc, ox, sub, own = places(k)

        def body(jj):
            j = lax.rem((1 - member) * half_chunks + jj, jnp.int32(chunks))
            here = rows_at(j, CHUNK)
            total = part[b, here, :].astype(jnp.float32)
            for dx in range(1, n_x):
                copy(part.at[b, here], x_in.at[dx - 1, sub, here], x_send.at[b, j], x_recv.at[dx - 1, sub, j],
                     tp=mate).wait_recv()
                total += x_in[dx - 1, sub, here, :].astype(jnp.float32)
            part[b, here, :] = total.astype(jnp.bfloat16)
            on(jj < half_chunks, lambda: q_copy(k, jj).start())

        on(own == tp, lambda: loop(0, chunks, body))

    def relay_down(k):
        d = flip(member, k, n_fs)

        def go():
            y_relay(DN0, d)
            y_relay(DN1, d)

        on(d > 0, go)

    def down_step(step):
        on(step < n_fs, lambda: relay_down(step))
        on(jnp.logical_and(step >= 1, step < n_fs + 1), lambda: down_one(step - 1))
        on(jnp.logical_and(step >= 2, step < n_fs + 2), lambda: across(step - 2))
        on(step >= 3, lambda: collect(step - 3))

    loop(0, n_fs + 3, down_step)

    for sub in range(per_own):
        b = tp * per_own + sub
        cols = slice(sub * block, (sub + 1) * block)

        def close(j, b=b, sub=sub, cols=cols):
            here = rows_at(j, CHUNK)
            copy(part.at[b, here], pair_in.at[sub, here], q_send.at[sub, j], q_recv.at[sub, j], fs=pair).wait_recv()
            mine = rows_at(member * half_chunks + j, CHUNK)
            total = part[b, mine, :].astype(jnp.float32) + pair_in[sub, here, :].astype(jnp.float32)
            total = (total * scale_all[1, sub]).astype(jnp.bfloat16).astype(jnp.float32)
            kept = resid_all[member, tp, here, cols].astype(jnp.float32)
            result_ref[here, cols] = (kept + total).astype(jnp.bfloat16)

        loop(0, half_chunks, close)

    for kind in range(KINDS):
        def sent(d, kind=kind):
            z_copy(kind, d).wait_send()
            for e in range(1, n_rep):
                y_copy(kind, d, e).wait_send()

        loop(1, n_fs, sent)

    def spans_sent(i):
        for kind in range(4):
            e_sent(kind, i)
        p_copy(i, member).wait_send()

    loop(0, spans, spans_sent)
    o_each(lambda d: o_copy(d).wait_send())
    s_each(lambda c: c.wait_send())

    def parts_sent(k):
        b, oc, ox, sub, own = places(k)

        def body(j):
            on(core != oc, lambda: m_copy(k, j).wait_send())
            on(jnp.logical_and(core == oc, xi != ox), lambda: x_copy(k, j).wait_send())
            on(jnp.logical_and(own == tp, j < half_chunks), lambda: q_copy(k, j).wait_send())

        loop(0, chunks, body)

    loop(0, n_fs, parts_sent)


def shards(
    sizes,
    tokens,
    pre_gain,
    u_weight,
    u_scale,
    v_weight,
    v_scale,
    group_gain,
    span_weight,
    span_bias,
    out_weight,
    out_scale,
    ffn_gain,
    gate_weight,
    gate_scale,
    up_weight,
    up_scale,
    down_weight,
    down_scale,
):
    n_rep, n_fs, n_tp = sizes
    n_x = n_tp // 2
    extra = (LANES - gate_weight.shape[1]) % (2 * LANES)
    if extra:
        gate_weight, up_weight = (jnp.pad(w, ((0, 0), (0, extra))) for w in (gate_weight, up_weight))
        gate_scale, up_scale = (jnp.pad(s, (0, extra)) for s in (gate_scale, up_scale))
        down_weight = jnp.pad(down_weight, ((0, extra), (0, 0)))
    rows, own_width = tokens.shape
    block, local_hidden = gate_weight.shape
    hid = local_hidden // 2
    channels = u_weight.shape[1]
    per_own = own_width // block
    spans = rows // span_weight.shape[1]
    chunks = 2 * rows // CHUNK
    row = lambda vector: vector.reshape(1, -1)
    operands = (
        tokens, u_weight, v_weight, out_weight, gate_weight, up_weight, down_weight, row(out_scale), row(down_scale),
        row(pre_gain), row(ffn_gain), row(u_scale), row(v_scale), row(group_gain), span_weight, span_bias,
        row(gate_scale), row(up_scale),
    )
    hbm, vmem = pl.BlockSpec(memory_space=pl.ANY), pl.BlockSpec(memory_space=pltpu.VMEM)
    bf16, f32 = jnp.bfloat16, jnp.float32
    dma = lambda *shape: pltpu.SemaphoreType.DMA(shape)
    return pl.pallas_call(
        functools.partial(layer_kernel, sizes),
        out_shape=jax.ShapeDtypeStruct((rows, own_width), bf16),
        in_specs=[hbm] * 7 + [vmem] * 11,
        out_specs=vmem,
        scratch_shapes=[
            pltpu.VMEM((block, channels), f32),
            pltpu.VMEM((block, channels), f32),
            pltpu.VMEM((channels, block), f32),
            pltpu.VMEM((block, local_hidden), f32),
            pltpu.VMEM((block, local_hidden), f32),
            pltpu.VMEM((local_hidden, block), f32),
            pltpu.VMEM((channels, block), bf16),
            pltpu.VMEM((2, block, 2 * hid), bf16),
            pltpu.VMEM((2, hid, block), bf16),
            pltpu.VMEM((n_tp, rows, own_width), bf16),
            pltpu.VMEM((n_fs, block, 2 * channels), bf16),
            pltpu.VMEM((n_tp, per_own, channels, block), bf16),
            pltpu.VMEM((2, per_own, 1, block), f32),
            pltpu.VMEM((n_tp, rows, channels), bf16),
            pltpu.VMEM((2, n_tp, rows, own_width), bf16),
            pltpu.VMEM((n_fs, 2 * rows, block), bf16),
            pltpu.VMEM((n_fs, block, 2 * hid), bf16),
            pltpu.VMEM((n_fs, hid, block), bf16),
            pltpu.VMEM((2 * rows, 2 * hid), f32),
            pltpu.VMEM((2 * rows, hid), bf16),
            pltpu.VMEM((n_fs, 2 * rows, block), bf16),
            pltpu.VMEM((n_x, per_own, 2 * rows, block), bf16),
            pltpu.VMEM((n_x - 1, per_own, 2 * rows, block), bf16),
            pltpu.VMEM((per_own, rows, block), bf16),
            dma(9),
            dma(KINDS, n_fs - 1),
            dma(KINDS, n_fs - 1),
            dma(KINDS, n_fs - 1, n_rep - 1),
            dma(KINDS, n_fs - 1, n_rep - 1),
            dma(4, spans, n_tp - 1),
            dma(4, spans, n_tp),
            dma(spans),
            dma(spans),
            dma(n_fs),
            dma(n_tp, per_own),
            dma(2, n_fs - 1),
            dma(2, per_own),
            dma(n_fs, chunks),
            dma(n_x, per_own, chunks),
            dma(n_fs, chunks),
            dma(n_x - 1, per_own, chunks),
            dma(per_own, chunks // 2),
            dma(per_own, chunks // 2),
        ],
        compiler_params=pltpu.CompilerParams(
            collective_id=0, has_side_effects=True, vmem_limit_bytes=63 * 1024 * 1024
        ),
    )(*operands)


def solution(mesh):
    placed = (
        P(("rep", "fs"), "tp"),
        P(),
        P("fs", "tp"),
        P("tp"),
        P("fs", "tp"),
        P("tp"),
        P("tp"),
        P("tp", None, None),
        P("tp", None),
        P("tp", "fs"),
        P("fs"),
        P(),
        P("fs", "tp"),
        P("tp"),
        P("fs", "tp"),
        P("tp"),
        P("tp", "fs"),
        P("fs"),
    )
    sizes = (mesh.shape["rep"], mesh.shape["fs"], mesh.shape["tp"])
    return jax.shard_map(
        functools.partial(shards, sizes), mesh=mesh, in_specs=placed, out_specs=P(("rep", "fs"), "tp"), check_vma=False
    )
```

```python
import functools

import jax
import jax.numpy as jnp
from jax import lax
from jax.experimental import pallas as pl
from jax.experimental.pallas import tpu as pltpu
from jax.sharding import PartitionSpec as P

EPS = 0.02
MESH = pl.DeviceIdType.MESH
LANES = 128
UV, OUT, GU0, GU1, DN = range(5)
TOK, GATED, OWN, PAIR = range(4)
CHUNK = 256


def on(condition, action):
    if isinstance(condition, bool):
        if condition:
            action()
    else:
        pl.when(condition)(action)


def flip(a, d, size):
    total, bit = 0, 1
    while bit < size:
        total = total + lax.rem(lax.div(a, jnp.int32(bit)) + lax.div(jnp.int32(d), jnp.int32(bit)), jnp.int32(2)) * bit
        bit *= 2
    return total


def loop(low, high, body):
    def step(i, carry):
        body(i)
        return carry

    lax.fori_loop(low, high, step, 0)


def layer_kernel(
    sizes,
    tokens_ref,
    u_ref,
    v_ref,
    out_ref,
    gate_ref,
    up_ref,
    down_ref,
    out_scale_ref,
    down_scale_ref,
    pre_gain_ref,
    ffn_gain_ref,
    u_scale_ref,
    v_scale_ref,
    group_gain_ref,
    span_ref,
    bias_ref,
    gate_scale_ref,
    up_scale_ref,
    result_ref,
    u_f,
    v_f,
    out_f,
    gate_f,
    up_f,
    down_f,
    gu_own,
    down_own,
    tok_all,
    uv_all,
    out_gather,
    out_all,
    scale_all,
    gated_all,
    resid_all,
    normed,
    gu_all,
    down_all,
    gu_acc,
    hidden,
    part,
    mate_in,
    x_in,
    pair_in,
    local_sem,
    z_send,
    z_recv,
    y_send,
    y_recv,
    e_send,
    e_recv,
    p_send,
    p_recv,
    o_send,
    o_recv,
    s_send,
    s_recv,
    m_send,
    m_recv,
    x_send,
    x_recv,
    q_send,
    q_recv,
):
    n_rep, n_fs, n_tp = sizes
    n_x = n_tp // 2
    rows, own_width = tokens_ref.shape
    block = gate_ref.shape[0]
    per_own = own_width // block
    hid = gate_ref.shape[1] // 2
    pieces, width_down = down_own.shape[1], down_own.shape[3]
    per_owner = per_own * pieces
    units = n_fs * pieces
    main = hid // LANES * LANES
    channels = u_ref.shape[1]
    groups, span = span_ref.shape[0], span_ref.shape[1]
    spans = rows // span
    total_rows = 2 * rows
    chunks = total_rows // CHUNK
    half_chunks = chunks // 2
    rep, fs, tp = lax.axis_index("rep"), lax.axis_index("fs"), lax.axis_index("tp")
    two = jnp.int32(2)
    member = lax.rem(fs, two)
    core, xi = lax.rem(tp, two), lax.div(tp, two)
    mate = tp + 1 - 2 * core
    pair = fs + 1 - 2 * member
    owner = lax.div(fs, jnp.int32(per_own))
    owner_sub = lax.rem(fs, jnp.int32(per_own))

    def copy(src, dst, send_sem, recv_sem, **device):
        return pltpu.make_async_remote_copy(
            src_ref=src, dst_ref=dst, send_sem=send_sem, recv_sem=recv_sem, device_id=device, device_id_type=MESH)

    def rows_at(i, size):
        return pl.ds(pl.multiple_of(i * size, size), size)

    def w_rows(kind, r):
        if kind in (GU0, GU1):
            size = block // n_rep // 2
            return pl.ds(pl.multiple_of((2 * r + (kind - GU0)) * size, size), size)
        size = (block if kind == UV else channels if kind == OUT else hid) // n_rep
        return pl.ds(pl.multiple_of(r * size, size), size)

    def w_slot(kind, f, r, p=0):
        if kind == DN:
            return down_all.at[f * pieces + p, w_rows(kind, r)]
        ref = uv_all if kind == UV else out_gather if kind == OUT else gu_all
        return ref.at[f, w_rows(kind, r)]

    def w_source(kind, g, p=0):
        if kind in (UV, OUT):
            return w_slot(kind, fs, rep)
        if kind == DN:
            return down_own.at[lax.rem(g, two), p, w_rows(kind, rep)]
        return gu_own.at[lax.rem(g, two), w_rows(kind, rep)]

    def z_copy(kind, d, p=0):
        g = flip(fs, d, n_fs)
        return copy(w_source(kind, g, p), w_slot(kind, fs, rep, p), z_send.at[kind + p, d - 1],
                    z_recv.at[kind + p, d - 1], fs=g)

    def y_copy(kind, d, e, p=0):
        slot = w_slot(kind, flip(fs, d, n_fs), rep, p)
        return copy(slot, slot, y_send.at[kind + p, d - 1, e - 1], y_recv.at[kind + p, d - 1, e - 1],
                    rep=lax.rem(rep + e, jnp.int32(n_rep)))

    def z_start(kind):
        def body(d):
            for p in range(pieces if kind == DN else 1):
                z_copy(kind, d, p).start()

        loop(1, n_fs, body)

    def y_relay(kind, d, p=0):
        slot = w_slot(kind, flip(fs, d, n_fs), rep, p)
        copy(slot, slot, z_send.at[kind + p, d - 1], z_recv.at[kind + p, d - 1], fs=pair).wait_recv()
        for e in range(1, n_rep):
            y_copy(kind, d, e, p).start()

    def y_ready(kind, d, p=0):
        for e in range(1, n_rep):
            slot = w_slot(kind, flip(fs, d, n_fs), lax.rem(rep - e + n_rep, jnp.int32(n_rep)), p)
            copy(slot, slot, y_send.at[kind + p, d - 1, e - 1], y_recv.at[kind + p, d - 1, e - 1],
                 rep=lax.rem(rep + 1, jnp.int32(n_rep))).wait_recv()

    def e_slot(kind, i, t):
        here = rows_at(i, span)
        if kind == TOK:
            return tok_all.at[t, here]
        if kind == GATED:
            return gated_all.at[t, here]
        return resid_all.at[member if kind == OWN else 1 - member, t, here]

    def x_peer(dx):
        return 2 * flip(xi, dx, n_x) + core

    def e_copy(kind, i, t, k, to):
        slot = e_slot(kind, i, t)
        return copy(slot, slot, e_send.at[kind, i, k], e_recv.at[kind, i, t], tp=to)

    def e_list(kind, i):
        out = [e_copy(kind, i, tp, 0, mate)]
        for dx in range(1, n_x):
            out.append(e_copy(kind, i, tp, dx, x_peer(dx)))
        return out

    def e_push(kind, i):
        for c in e_list(kind, i):
            c.start()

    def e_wait(kind, i, t):
        e_copy(kind, i, t, 0, mate).wait_recv()

    def e_relay(kind, i):
        for dx in range(1, n_x):
            e_wait(kind, i, x_peer(dx))
            e_copy(kind, i, x_peer(dx), n_x - 1 + dx, mate).start()

    def e_finish(kind, i):
        for dx in range(n_x):
            e_wait(kind, i, 2 * flip(xi, dx, n_x) + 1 - core)

    def e_sent(kind, i):
        for c in e_list(kind, i):
            c.wait_send()
        for dx in range(1, n_x):
            e_copy(kind, i, x_peer(dx), n_x - 1 + dx, mate).wait_send()

    def p_copy(i, which):
        slot = resid_all.at[which, tp, rows_at(i, span)]
        return copy(slot, slot, p_send.at[i], p_recv.at[i], fs=pair)

    def o_copy(k, sub):
        to = lax.rem(tp + k, jnp.int32(n_tp))
        return copy(out_gather.at[to * per_own + sub], out_all.at[tp, sub], o_send.at[k - 1, sub],
                    o_recv.at[k - 1, sub], tp=to)

    def o_take(k, sub):
        sender = lax.rem(tp - k + n_tp, jnp.int32(n_tp))
        copy(out_gather.at[0], out_all.at[sender, sub], o_send.at[k - 1, sub], o_recv.at[k - 1, sub],
             tp=mate).wait_recv()

    def o_each(action):
        for k in range(1, n_tp):
            for sub in range(per_own):
                action(k, sub)

    def s_copy(d, which):
        g = flip(fs, d, n_fs)
        src = (out_scale_ref, down_scale_ref)[which]
        return copy(src, scale_all.at[which, owner_sub], s_send.at[which, d - 1], s_recv.at[which, owner_sub], fs=g)

    loads = [
        pltpu.make_async_copy(src, dst, local_sem.at[i])
        for i, (src, dst) in enumerate((
            (tokens_ref, tok_all.at[tp]), (u_ref, u_f), (v_ref, v_f), (out_ref, out_f), (gate_ref, gate_f),
            (up_ref, up_f), (down_ref, down_f)))
    ]
    for load in loads:
        load.start()

    barrier = pltpu.get_barrier_semaphore()

    def greet(**device):
        pl.semaphore_signal(barrier, inc=1, device_id=device, device_id_type=MESH)

    for k in range(1, n_tp):
        greet(tp=lax.rem(tp + k, jnp.int32(n_tp)))
    loop(1, n_fs, lambda d: greet(fs=flip(fs, d, n_fs)))
    for e in range(1, n_rep):
        greet(rep=lax.rem(rep + e, jnp.int32(n_rep)))
    pl.semaphore_wait(barrier, n_tp + n_fs + n_rep - 3)

    loads[0].wait()
    loop(0, spans, lambda i: e_push(TOK, i))
    loads[1].wait()
    loads[2].wait()
    uv_all[fs, :, 0:channels] = u_f[...].astype(jnp.bfloat16)
    uv_all[fs, :, channels:2 * channels] = v_f[...].astype(jnp.bfloat16)
    z_start(UV)
    loads[3].wait()
    out_gather[fs] = out_f[...].astype(jnp.bfloat16)
    z_start(OUT)

    def keep_own():
        scale_all[0, owner_sub] = out_scale_ref[...]
        scale_all[1, owner_sub] = down_scale_ref[...]

    on(owner == tp, keep_own)

    def s_each(action):
        def body(d):
            for which in range(2):
                action(s_copy(d, which))

        on(owner == tp, lambda: loop(1, n_fs, body))

    s_each(lambda c: c.start())

    low = lax.broadcasted_iota(jnp.int32, (1, LANES), 1) < LANES // 2
    unit = 64

    def swap(value):
        return pltpu.roll(value, LANES // 2, 1)

    loads[4].wait()
    loads[5].wait()

    def cast_gu(i):
        here = rows_at(i, unit)
        for member_of in range(2):
            first = member_of * (main + LANES)
            gu_own[member_of, here, 0:main] = gate_f[here, first:first + main].astype(jnp.bfloat16)
            gu_own[member_of, here, main:2 * main] = up_f[here, first:first + main].astype(jnp.bfloat16)
        g, u = gate_f[here, main:main + LANES], up_f[here, main:main + LANES]
        gu_own[0, here, 2 * main:] = jnp.where(low, g, swap(u)).astype(jnp.bfloat16)
        gu_own[1, here, 2 * main:] = jnp.where(low, swap(g), u).astype(jnp.bfloat16)

    loop(0, block // unit, cast_gu)
    z_start(GU0)
    keep_gu = pltpu.make_async_copy(gu_own.at[member], gu_all.at[fs], local_sem.at[7])
    keep_gu.start()
    loads[6].wait()

    def cast_down(i):
        here = rows_at(i, unit)
        there = rows_at(jnp.where(i < main // unit, i + (main + LANES) // unit, main // unit + 1), unit)
        for p in range(pieces):
            cols = slice(p * width_down, (p + 1) * width_down)
            down_own[0, p, here] = down_f[here, cols].astype(jnp.bfloat16)
            down_own[1, p, here] = down_f[there, cols].astype(jnp.bfloat16)

    loop(0, hid // unit, cast_down)
    keep_down = pltpu.make_async_copy(down_own.at[member], down_all.at[pl.ds(fs * pieces, pieces)], local_sem.at[8])
    keep_down.start()

    loop(0, spans, lambda i: e_relay(TOK, i))
    loop(1, n_fs, lambda d: y_relay(UV, d))
    loop(1, n_fs, lambda d: y_relay(OUT, d))
    loop(1, n_fs, lambda d: y_ready(UV, d))

    eye = lax.broadcasted_iota(jnp.int32, (span, span), 0) == lax.broadcasted_iota(jnp.int32, (span, span), 1)
    tril = lax.broadcasted_iota(jnp.int32, (span, span), 0) >= lax.broadcasted_iota(jnp.int32, (span, span), 1)

    def mixer_span(i):
        e_finish(TOK, i)
        here = rows_at(i, span)
        square = jnp.zeros((span, 1), jnp.float32)
        for t in range(n_tp):
            wide = tok_all[t, here, :].astype(jnp.float32)
            square += jnp.sum(wide * wide, axis=-1, keepdims=True)
        inverse = lax.rsqrt(square / (n_tp * own_width) + EPS)
        pre = None
        for f in range(n_fs):
            t, sub = f // per_own, f % per_own
            wide = tok_all[t, here, sub * block:(sub + 1) * block].astype(jnp.float32)
            source = (wide * inverse * pre_gain_ref[:, f * block:(f + 1) * block]).astype(jnp.bfloat16)
            term = jnp.dot(source, uv_all[f], preferred_element_type=jnp.float32)
            pre = term if f == 0 else pre + term
        u_act = jax.nn.gelu(pre[:, :channels] * u_scale_ref[...])
        v_act = jax.nn.gelu(pre[:, channels:] * v_scale_ref[...])
        width = channels // groups
        group_of = lax.broadcasted_iota(jnp.int32, v_act.shape, 1) // width
        centre = jnp.zeros_like(v_act)
        for g in range(groups):
            mean = jnp.sum(jnp.where(group_of == g, v_act, 0.0), axis=-1, keepdims=True) / width
            centre = jnp.where(group_of == g, mean, centre)
        apart = v_act - centre
        square = apart * apart
        inverse = jnp.zeros_like(v_act)
        for g in range(groups):
            spread = jnp.sum(jnp.where(group_of == g, square, 0.0), axis=-1, keepdims=True) / width
            inverse = jnp.where(group_of == g, lax.rsqrt(spread + EPS), inverse)
        v_norm = (apart * inverse * group_gain_ref[...]).astype(jnp.bfloat16)
        mixed = jnp.zeros_like(v_act)
        for g in range(groups):
            lower = jnp.where(tril, span_ref[g].astype(jnp.float32), 0.0).astype(jnp.bfloat16)
            bias = jnp.sum(jnp.where(eye, bias_ref[g:g + 1, :], 0.0), axis=1, keepdims=True)
            term = jnp.dot(lower, v_norm, preferred_element_type=jnp.float32) + bias
            mixed = jnp.where(group_of == g, term, mixed)
        gated_all[tp, here, :] = (u_act * mixed).astype(jnp.bfloat16)
        e_push(GATED, i)

    loop(0, spans, mixer_span)
    loop(1, n_fs, lambda d: y_ready(OUT, d))
    o_each(lambda k, sub: o_copy(k, sub).start())
    for sub in range(per_own):
        out_all[tp, sub] = out_gather[tp * per_own + sub]
    loop(0, spans, lambda i: e_relay(GATED, i))

    o_each(o_take)

    def scale_arrived(sub):
        def take():
            for which in range(2):
                copy(out_scale_ref, scale_all.at[which, sub], s_send.at[which, 0], s_recv.at[which, sub],
                     fs=pair).wait_recv()

        on(tp * per_own + sub != fs, take)

    loop(0, per_own, scale_arrived)

    def resid_span(i):
        e_finish(GATED, i)
        here = rows_at(i, span)
        for sub in range(per_own):
            mix = None
            for s in range(n_tp):
                term = jnp.dot(gated_all[s, here, :], out_all[s, sub], preferred_element_type=jnp.float32)
                mix = term if s == 0 else mix + term
            mix = (mix * scale_all[0, sub]).astype(jnp.bfloat16)
            cols = slice(sub * block, (sub + 1) * block)
            resid_all[member, tp, here, cols] = (
                tok_all[tp, here, cols].astype(jnp.float32) + mix.astype(jnp.float32)).astype(jnp.bfloat16)
        e_push(OWN, i)
        p_copy(i, member).start()

    loop(0, spans, resid_span)
    z_start(GU1)
    z_start(DN)

    def norm_span(which, i):
        here = rows_at(i, span)
        square = jnp.zeros((span, 1), jnp.float32)
        for t in range(n_tp):
            wide = resid_all[which, t, here, :].astype(jnp.float32)
            square += jnp.sum(wide * wide, axis=-1, keepdims=True)
        inverse = lax.rsqrt(square / (n_tp * own_width) + EPS)
        there = rows_at(which * spans + i, span)
        for f in range(n_fs):
            t, sub = f // per_own, f % per_own
            wide = resid_all[which, t, here, sub * block:(sub + 1) * block].astype(jnp.float32)
            gain = ffn_gain_ref[:, f * block:(f + 1) * block]
            normed[f, there, :] = (wide * inverse * gain).astype(jnp.bfloat16)

    loop(0, spans, lambda i: e_relay(OWN, i))

    def own_span(i):
        e_finish(OWN, i)
        norm_span(member, i)

    loop(0, spans, own_span)
    loop(1, n_fs, lambda d: y_relay(GU0, d))

    def pair_span(i):
        p_copy(i, 1 - member).wait_recv()
        e_push(PAIR, i)

    loop(0, spans, pair_span)
    loop(0, spans, lambda i: e_relay(PAIR, i))

    def other_span(i):
        e_finish(PAIR, i)
        norm_span(1 - member, i)

    loop(0, spans, other_span)

    keep_gu.wait()

    def first_gu(i):
        here = rows_at(i, CHUNK)
        gu_acc[here, :] = jnp.dot(normed[fs, here, :], gu_all[fs], preferred_element_type=jnp.float32)

    loop(0, chunks, first_gu)

    def fold_gu(d):
        y_ready(GU0, d)
        y_ready(GU1, d)
        f = flip(fs, d, n_fs)

        def body(i):
            here = rows_at(i, CHUNK)
            gu_acc[here, :] += jnp.dot(normed[f, here, :], gu_all[f], preferred_element_type=jnp.float32)

        loop(0, chunks, body)

    def gu_step(d):
        on(d < n_fs, lambda: y_relay(GU1, d))
        on(d > 1, lambda: fold_gu(d - 1))

    loop(1, n_fs + 1, gu_step)

    second = member == 1

    def hidden_chunk(i):
        here = rows_at(i, 64)
        tiles = main // LANES
        for j in range(tiles):
            gate_scale = jnp.where(second, gate_scale_ref[tiles + 1 + j:tiles + 2 + j], gate_scale_ref[j:j + 1])
            up_scale = jnp.where(second, up_scale_ref[tiles + 1 + j:tiles + 2 + j], up_scale_ref[j:j + 1])
            a = gu_acc[here, j * LANES:(j + 1) * LANES] * gate_scale
            b = gu_acc[here, main + j * LANES:main + (j + 1) * LANES] * up_scale
            hidden[here, j * LANES:(j + 1) * LANES] = (a / (1.0 + jnp.exp(-a)) * b).astype(jnp.bfloat16)
        gs, us = gate_scale_ref[tiles:tiles + 1], up_scale_ref[tiles:tiles + 1]
        a = gu_acc[here, 2 * main:] * jnp.where(second, jnp.where(low, swap(gs), us), jnp.where(low, gs, swap(us)))
        b = swap(a)
        last = (a / (1.0 + jnp.exp(-a)) * b).astype(jnp.bfloat16)
        hidden[here, main:hid] = last[:, 0:hid - main]

    loop(0, total_rows // 64, hidden_chunk)
    keep_down.wait()

    def places(s):
        d, p = lax.div(s, jnp.int32(pieces)), lax.rem(s, jnp.int32(pieces))
        b = flip(fs, d, n_fs)
        own = lax.div(b, jnp.int32(per_own))
        sub = lax.rem(b, jnp.int32(per_own)) * pieces + p
        return b * pieces + p, lax.rem(own, two), lax.div(own, two), sub, own

    def m_copy(k, j):
        b, oc, ox, sub, own = places(k)
        here = rows_at(j, CHUNK)
        return copy(part.at[b, here], mate_in.at[ox, sub, here], m_send.at[b, j], m_recv.at[ox, sub, j], tp=mate)

    def x_copy(k, j):
        b, oc, ox, sub, own = places(k)
        here = rows_at(j, CHUNK)
        d = flip(xi, ox, n_x)
        return copy(part.at[b, here], x_in.at[d - 1, sub, here], x_send.at[b, j], x_recv.at[d - 1, sub, j], tp=own)

    def q_copy(k, j):
        b, oc, ox, sub, own = places(k)
        src = part.at[b, rows_at((1 - member) * half_chunks + j, CHUNK)]
        return copy(src, pair_in.at[sub, rows_at(j, CHUNK)], q_send.at[sub, j], q_recv.at[sub, j], fs=pair)

    def down_one(k):
        b, oc, ox, sub, own = places(k)
        d, p = lax.div(k, jnp.int32(pieces)), lax.rem(k, jnp.int32(pieces))
        on(d > 0, lambda: y_ready(DN, d, p))

        def body(j):
            here = rows_at(j, CHUNK)
            part[b, here, :] = jnp.dot(hidden[here, :], down_all[b], preferred_element_type=jnp.float32).astype(
                jnp.bfloat16)
            on(core != oc, lambda: m_copy(k, j).start())

        loop(0, chunks, body)

    def across(k):
        b, oc, ox, sub, own = places(k)

        def body(j):
            here = rows_at(j, CHUNK)
            m_copy(k, j).wait_recv()
            part[b, here, :] = (part[b, here, :].astype(jnp.float32)
                                + mate_in[ox, sub, here, :].astype(jnp.float32)).astype(jnp.bfloat16)
            on(xi != ox, lambda: x_copy(k, j).start())

        on(core == oc, lambda: loop(0, chunks, body))

    def collect(k):
        b, oc, ox, sub, own = places(k)

        def body(jj):
            j = lax.rem((1 - member) * half_chunks + jj, jnp.int32(chunks))
            here = rows_at(j, CHUNK)
            total = part[b, here, :].astype(jnp.float32)
            for dx in range(1, n_x):
                copy(part.at[b, here], x_in.at[dx - 1, sub, here], x_send.at[b, j], x_recv.at[dx - 1, sub, j],
                     tp=mate).wait_recv()
                total += x_in[dx - 1, sub, here, :].astype(jnp.float32)
            part[b, here, :] = total.astype(jnp.bfloat16)
            on(jj < half_chunks, lambda: q_copy(k, jj).start())

        on(own == tp, lambda: loop(0, chunks, body))

    def relay_down(k):
        d, p = lax.div(k, jnp.int32(pieces)), lax.rem(k, jnp.int32(pieces))
        on(d > 0, lambda: y_relay(DN, d, p))

    def down_step(step):
        on(step < units, lambda: relay_down(step))
        on(jnp.logical_and(step >= 1, step < units + 1), lambda: down_one(step - 1))
        on(jnp.logical_and(step >= 2, step < units + 2), lambda: across(step - 2))
        on(step >= 3, lambda: collect(step - 3))

    loop(0, units + 3, down_step)

    for sub in range(per_owner):
        b = tp * per_owner + sub
        cols = slice(sub * width_down, (sub + 1) * width_down)

        def close(j, b=b, sub=sub, cols=cols):
            here = rows_at(j, CHUNK)
            copy(part.at[b, here], pair_in.at[sub, here], q_send.at[sub, j], q_recv.at[sub, j], fs=pair).wait_recv()
            mine = rows_at(member * half_chunks + j, CHUNK)
            total = part[b, mine, :].astype(jnp.float32) + pair_in[sub, here, :].astype(jnp.float32)
            total = (total * scale_all[1, sub // pieces, :, sub % pieces * width_down:(sub % pieces + 1) * width_down]).astype(jnp.bfloat16).astype(jnp.float32)
            kept = resid_all[member, tp, here, cols].astype(jnp.float32)
            result_ref[here, cols] = (kept + total).astype(jnp.bfloat16)

        loop(0, half_chunks, close)

    for kind in range(5):
        def sent(d, kind=kind):
            for p in range(pieces if kind == DN else 1):
                z_copy(kind, d, p).wait_send()
                for e in range(1, n_rep):
                    y_copy(kind, d, e, p).wait_send()

        loop(1, n_fs, sent)

    def spans_sent(i):
        for kind in range(4):
            e_sent(kind, i)
        p_copy(i, member).wait_send()

    loop(0, spans, spans_sent)
    o_each(lambda k, sub: o_copy(k, sub).wait_send())
    s_each(lambda c: c.wait_send())

    def parts_sent(k):
        b, oc, ox, sub, own = places(k)

        def body(j):
            on(core != oc, lambda: m_copy(k, j).wait_send())
            on(jnp.logical_and(core == oc, xi != ox), lambda: x_copy(k, j).wait_send())
            on(jnp.logical_and(own == tp, j < half_chunks), lambda: q_copy(k, j).wait_send())

        loop(0, chunks, body)

    loop(0, units, parts_sent)


def shards(
    sizes,
    tokens,
    pre_gain,
    u_weight,
    u_scale,
    v_weight,
    v_scale,
    group_gain,
    span_weight,
    span_bias,
    out_weight,
    out_scale,
    ffn_gain,
    gate_weight,
    gate_scale,
    up_weight,
    up_scale,
    down_weight,
    down_scale,
):
    n_rep, n_fs, n_tp = sizes
    n_x = n_tp // 2
    extra = (LANES - gate_weight.shape[1]) % (2 * LANES)
    if extra:
        gate_weight, up_weight = (jnp.pad(w, ((0, 0), (0, extra))) for w in (gate_weight, up_weight))
        gate_scale, up_scale = (jnp.pad(s, (0, extra)) for s in (gate_scale, up_scale))
        down_weight = jnp.pad(down_weight, ((0, extra), (0, 0)))
    rows, own_width = tokens.shape
    block, local_hidden = gate_weight.shape
    hid = local_hidden // 2
    channels = u_weight.shape[1]
    per_own = own_width // block
    spans = rows // span_weight.shape[1]
    chunks = 2 * rows // CHUNK
    pieces = max(block // (2 * LANES), 1)
    width_down, per_owner, units = block // pieces, per_own * pieces, n_fs * pieces
    row = lambda vector: vector.reshape(1, -1)
    operands = (
        tokens, u_weight, v_weight, out_weight, gate_weight, up_weight, down_weight, row(out_scale), row(down_scale),
        row(pre_gain), row(ffn_gain), row(u_scale), row(v_scale), row(group_gain), span_weight, span_bias,
        gate_scale.reshape(-1, LANES), up_scale.reshape(-1, LANES),
    )
    hbm, vmem = pl.BlockSpec(memory_space=pl.ANY), pl.BlockSpec(memory_space=pltpu.VMEM)
    bf16, f32 = jnp.bfloat16, jnp.float32
    dma = lambda *shape: pltpu.SemaphoreType.DMA(shape)
    return pl.pallas_call(
        functools.partial(layer_kernel, sizes),
        out_shape=jax.ShapeDtypeStruct((rows, own_width), bf16),
        in_specs=[hbm] * 7 + [vmem] * 11,
        out_specs=vmem,
        scratch_shapes=[
            pltpu.VMEM((block, channels), f32),
            pltpu.VMEM((block, channels), f32),
            pltpu.VMEM((channels, block), f32),
            pltpu.VMEM((block, local_hidden), f32),
            pltpu.VMEM((block, local_hidden), f32),
            pltpu.VMEM((local_hidden, block), f32),
            pltpu.VMEM((2, block, 2 * hid), bf16),
            pltpu.VMEM((2, pieces, hid, width_down), bf16),
            pltpu.VMEM((n_tp, rows, own_width), bf16),
            pltpu.VMEM((n_fs, block, 2 * channels), bf16),
            pltpu.VMEM((n_fs, channels, block), bf16),
            pltpu.VMEM((n_tp, per_own, channels, block), bf16),
            pltpu.VMEM((2, per_own, 1, block), f32),
            pltpu.VMEM((n_tp, rows, channels), bf16),
            pltpu.VMEM((2, n_tp, rows, own_width), bf16),
            pltpu.VMEM((n_fs, 2 * rows, block), bf16),
            pltpu.VMEM((n_fs, block, 2 * hid), bf16),
            pltpu.VMEM((units, hid, width_down), bf16),
            pltpu.VMEM((2 * rows, 2 * hid), f32),
            pltpu.VMEM((2 * rows, hid), bf16),
            pltpu.VMEM((units, 2 * rows, width_down), bf16),
            pltpu.VMEM((n_x, per_owner, 2 * rows, width_down), bf16),
            pltpu.VMEM((n_x - 1, per_owner, 2 * rows, width_down), bf16),
            pltpu.VMEM((per_owner, rows, width_down), bf16),
            dma(9),
            dma(DN + pieces, n_fs - 1),
            dma(DN + pieces, n_fs - 1),
            dma(DN + pieces, n_fs - 1, n_rep - 1),
            dma(DN + pieces, n_fs - 1, n_rep - 1),
            dma(4, spans, n_tp - 1),
            dma(4, spans, n_tp),
            dma(spans),
            dma(spans),
            dma(n_tp - 1, per_own),
            dma(n_tp - 1, per_own),
            dma(2, n_fs - 1),
            dma(2, per_own),
            dma(units, chunks),
            dma(n_x, per_owner, chunks),
            dma(units, chunks),
            dma(n_x - 1, per_owner, chunks),
            dma(per_owner, chunks // 2),
            dma(per_owner, chunks // 2),
        ],
        compiler_params=pltpu.CompilerParams(
            collective_id=0, has_side_effects=True, vmem_limit_bytes=63 * 1024 * 1024
        ),
    )(*operands)


def solution(mesh):
    placed = (
        P(("rep", "fs"), "tp"),
        P(),
        P("fs", "tp"),
        P("tp"),
        P("fs", "tp"),
        P("tp"),
        P("tp"),
        P("tp", None, None),
        P("tp", None),
        P("tp", "fs"),
        P("fs"),
        P(),
        P("fs", "tp"),
        P("tp"),
        P("fs", "tp"),
        P("tp"),
        P("tp", "fs"),
        P("fs"),
    )
    sizes = (mesh.shape["rep"], mesh.shape["fs"], mesh.shape["tp"])
    return jax.shard_map(
        functools.partial(shards, sizes), mesh=mesh, in_specs=placed, out_specs=P(("rep", "fs"), "tp"), check_vma=False
    )
```

```python
import functools

import jax
import jax.numpy as jnp
from jax import lax
from jax.experimental import pallas as pl
from jax.experimental.pallas import tpu as pltpu
from jax.sharding import PartitionSpec as P

EPS = 0.02
MESH = pl.DeviceIdType.MESH
LANES = 128
CUTS = 8
UV, OUT, GU, DN = 0, 1, 2, 2 + CUTS
TOK, GATED, OWN, PAIR = range(4)
CHUNK = 256


def on(condition, action):
    if isinstance(condition, bool):
        if condition:
            action()
    else:
        pl.when(condition)(action)


def flip(a, d, size):
    total, bit = 0, 1
    while bit < size:
        total = total + lax.rem(lax.div(a, jnp.int32(bit)) + lax.div(jnp.int32(d), jnp.int32(bit)), jnp.int32(2)) * bit
        bit *= 2
    return total


def loop(low, high, body):
    def step(i, carry):
        body(i)
        return carry

    lax.fori_loop(low, high, step, 0)


def layer_kernel(
    sizes,
    tokens_ref,
    u_ref,
    v_ref,
    out_ref,
    gate_ref,
    up_ref,
    down_ref,
    out_scale_ref,
    down_scale_ref,
    pre_gain_ref,
    ffn_gain_ref,
    u_scale_ref,
    v_scale_ref,
    group_gain_ref,
    span_ref,
    bias_ref,
    gate_scale_ref,
    up_scale_ref,
    result_ref,
    u_f,
    v_f,
    out_f,
    gate_f,
    up_f,
    down_f,
    gu_own,
    down_own,
    tok_all,
    uv_all,
    out_gather,
    out_all,
    scale_all,
    gated_all,
    resid_all,
    normed,
    gu_all,
    down_all,
    gu_acc,
    hidden,
    part,
    mate_in,
    x_in,
    pair_in,
    local_sem,
    z_send,
    z_recv,
    y_send,
    y_recv,
    e_send,
    e_recv,
    p_send,
    p_recv,
    o_send,
    o_recv,
    s_send,
    s_recv,
    m_send,
    m_recv,
    x_send,
    x_recv,
    q_send,
    q_recv,
):
    n_rep, n_fs, n_tp = sizes
    n_x = n_tp // 2
    rows, own_width = tokens_ref.shape
    block = gate_ref.shape[0]
    per_own = own_width // block
    hid = gate_ref.shape[1] // 2
    cuts = min(CUTS, block // n_rep // 16)
    early_cuts = cuts // 2
    pieces, width_down = down_own.shape[1], down_own.shape[3]
    per_owner = per_own * pieces
    units = n_fs * pieces
    main = hid // LANES * LANES
    channels = u_ref.shape[1]
    groups, span = span_ref.shape[0], span_ref.shape[1]
    spans = rows // span
    total_rows = 2 * rows
    chunks = total_rows // CHUNK
    half_chunks = chunks // 2
    rep, fs, tp = lax.axis_index("rep"), lax.axis_index("fs"), lax.axis_index("tp")
    two = jnp.int32(2)
    member = lax.rem(fs, two)
    core, xi = lax.rem(tp, two), lax.div(tp, two)
    mate = tp + 1 - 2 * core
    pair = fs + 1 - 2 * member
    owner = lax.div(fs, jnp.int32(per_own))
    owner_sub = lax.rem(fs, jnp.int32(per_own))

    def copy(src, dst, send_sem, recv_sem, **device):
        return pltpu.make_async_remote_copy(
            src_ref=src, dst_ref=dst, send_sem=send_sem, recv_sem=recv_sem, device_id=device, device_id_type=MESH)

    def rows_at(i, size):
        return pl.ds(pl.multiple_of(i * size, size), size)

    def w_rows(kind, r, p=0):
        if kind == GU:
            size = block // n_rep // cuts
            return pl.ds(pl.multiple_of((cuts * r + p) * size, size), size)
        size = (block if kind == UV else channels if kind == OUT else hid) // n_rep
        return pl.ds(pl.multiple_of(r * size, size), size)

    def w_slot(kind, f, r, p=0):
        if kind == DN:
            return down_all.at[f * pieces + p, w_rows(kind, r)]
        ref = uv_all if kind == UV else out_gather if kind == OUT else gu_all
        return ref.at[f, w_rows(kind, r, p)]

    def w_source(kind, g, p=0):
        if kind in (UV, OUT):
            return w_slot(kind, fs, rep)
        if kind == DN:
            return down_own.at[lax.rem(g, two), p, w_rows(kind, rep)]
        return gu_own.at[lax.rem(g, two), w_rows(kind, rep, p)]

    def z_copy(kind, d, p=0):
        g = flip(fs, d, n_fs)
        return copy(w_source(kind, g, p), w_slot(kind, fs, rep, p), z_send.at[kind + p, d - 1],
                    z_recv.at[kind + p, d - 1], fs=g)

    def y_copy(kind, d, e, p=0):
        slot = w_slot(kind, flip(fs, d, n_fs), rep, p)
        return copy(slot, slot, y_send.at[kind + p, d - 1, e - 1], y_recv.at[kind + p, d - 1, e - 1],
                    rep=lax.rem(rep + e, jnp.int32(n_rep)))

    def z_start(kind, low=0, high=1):
        def body(d):
            for p in range(low, high):
                z_copy(kind, d, p).start()

        loop(1, n_fs, body)

    def unit_at(k):
        k = jnp.int32(k)
        return lax.div(k, jnp.int32(pieces)), lax.rem(k, jnp.int32(pieces))

    def y_relay(kind, d, p=0):
        slot = w_slot(kind, flip(fs, d, n_fs), rep, p)
        copy(slot, slot, z_send.at[kind + p, d - 1], z_recv.at[kind + p, d - 1], fs=pair).wait_recv()
        for e in range(1, n_rep):
            y_copy(kind, d, e, p).start()

    def y_ready(kind, d, p=0):
        for e in range(1, n_rep):
            slot = w_slot(kind, flip(fs, d, n_fs), lax.rem(rep - e + n_rep, jnp.int32(n_rep)), p)
            copy(slot, slot, y_send.at[kind + p, d - 1, e - 1], y_recv.at[kind + p, d - 1, e - 1],
                 rep=lax.rem(rep + 1, jnp.int32(n_rep))).wait_recv()

    def e_slot(kind, i, t):
        here = rows_at(i, span)
        if kind == TOK:
            return tok_all.at[t, here]
        if kind == GATED:
            return gated_all.at[t, here]
        return resid_all.at[member if kind == OWN else 1 - member, t, here]

    def x_peer(dx):
        return 2 * flip(xi, dx, n_x) + core

    def e_copy(kind, i, t, k, to):
        slot = e_slot(kind, i, t)
        return copy(slot, slot, e_send.at[kind, i, k], e_recv.at[kind, i, t], tp=to)

    def e_list(kind, i):
        out = [e_copy(kind, i, tp, 0, mate)]
        for dx in range(1, n_x):
            out.append(e_copy(kind, i, tp, dx, x_peer(dx)))
        return out

    def e_push(kind, i):
        for c in e_list(kind, i):
            c.start()

    def e_wait(kind, i, t):
        e_copy(kind, i, t, 0, mate).wait_recv()

    def e_relay(kind, i):
        for dx in range(1, n_x):
            e_wait(kind, i, x_peer(dx))
            e_copy(kind, i, x_peer(dx), n_x - 1 + dx, mate).start()

    def e_finish(kind, i):
        for dx in range(n_x):
            e_wait(kind, i, 2 * flip(xi, dx, n_x) + 1 - core)

    def e_sent(kind, i):
        for c in e_list(kind, i):
            c.wait_send()
        for dx in range(1, n_x):
            e_copy(kind, i, x_peer(dx), n_x - 1 + dx, mate).wait_send()

    def p_copy(i, which):
        slot = resid_all.at[which, tp, rows_at(i, span)]
        return copy(slot, slot, p_send.at[i], p_recv.at[i], fs=pair)

    def o_copy(k, sub):
        to = lax.rem(tp + k, jnp.int32(n_tp))
        return copy(out_gather.at[to * per_own + sub], out_all.at[tp, sub], o_send.at[k - 1, sub],
                    o_recv.at[k - 1, sub], tp=to)

    def o_take(k, sub):
        sender = lax.rem(tp - k + n_tp, jnp.int32(n_tp))
        copy(out_gather.at[0], out_all.at[sender, sub], o_send.at[k - 1, sub], o_recv.at[k - 1, sub],
             tp=mate).wait_recv()

    def o_each(action):
        for k in range(1, n_tp):
            for sub in range(per_own):
                action(k, sub)

    def s_copy(d, which):
        g = flip(fs, d, n_fs)
        src = (out_scale_ref, down_scale_ref)[which]
        return copy(src, scale_all.at[which, owner_sub], s_send.at[which, d - 1], s_recv.at[which, owner_sub], fs=g)

    loads = [
        pltpu.make_async_copy(src, dst, local_sem.at[i])
        for i, (src, dst) in enumerate((
            (tokens_ref, tok_all.at[tp]), (u_ref, u_f), (v_ref, v_f), (out_ref, out_f), (gate_ref, gate_f),
            (up_ref, up_f), (down_ref, down_f)))
    ]
    for load in loads:
        load.start()

    barrier = pltpu.get_barrier_semaphore()

    def greet(**device):
        pl.semaphore_signal(barrier, inc=1, device_id=device, device_id_type=MESH)

    for k in range(1, n_tp):
        greet(tp=lax.rem(tp + k, jnp.int32(n_tp)))
    loop(1, n_fs, lambda d: greet(fs=flip(fs, d, n_fs)))
    for e in range(1, n_rep):
        greet(rep=lax.rem(rep + e, jnp.int32(n_rep)))
    pl.semaphore_wait(barrier, n_tp + n_fs + n_rep - 3)

    loads[0].wait()
    loop(0, spans, lambda i: e_push(TOK, i))
    loads[1].wait()
    loads[2].wait()
    uv_all[fs, :, 0:channels] = u_f[...].astype(jnp.bfloat16)
    uv_all[fs, :, channels:2 * channels] = v_f[...].astype(jnp.bfloat16)
    z_start(UV)
    loads[3].wait()
    out_gather[fs] = out_f[...].astype(jnp.bfloat16)
    z_start(OUT)

    def keep_own():
        scale_all[0, owner_sub] = out_scale_ref[...]
        scale_all[1, owner_sub] = down_scale_ref[...]

    on(owner == tp, keep_own)

    def s_each(action):
        def body(d):
            for which in range(2):
                action(s_copy(d, which))

        on(owner == tp, lambda: loop(1, n_fs, body))

    s_each(lambda c: c.start())

    low = lax.broadcasted_iota(jnp.int32, (1, LANES), 1) < LANES // 2
    unit = 64

    def swap(value):
        return pltpu.roll(value, LANES // 2, 1)

    loads[4].wait()
    loads[5].wait()

    def cast_gu(i):
        here = rows_at(i, unit)
        for member_of in range(2):
            first = member_of * (main + LANES)
            gu_own[member_of, here, 0:main] = gate_f[here, first:first + main].astype(jnp.bfloat16)
            gu_own[member_of, here, main:2 * main] = up_f[here, first:first + main].astype(jnp.bfloat16)
        g, u = gate_f[here, main:main + LANES], up_f[here, main:main + LANES]
        gu_own[0, here, 2 * main:] = jnp.where(low, g, swap(u)).astype(jnp.bfloat16)
        gu_own[1, here, 2 * main:] = jnp.where(low, swap(g), u).astype(jnp.bfloat16)

    loop(0, block // unit, cast_gu)
    for p in range(early_cuts):
        z_start(GU, p, p + 1)
    keep_gu = pltpu.make_async_copy(gu_own.at[member], gu_all.at[fs], local_sem.at[7])
    keep_gu.start()
    loads[6].wait()

    def cast_down(i):
        here = rows_at(i, unit)
        there = rows_at(jnp.where(i < main // unit, i + (main + LANES) // unit, main // unit + 1), unit)
        for p in range(pieces):
            cols = slice(p * width_down, (p + 1) * width_down)
            down_own[0, p, here] = down_f[here, cols].astype(jnp.bfloat16)
            down_own[1, p, here] = down_f[there, cols].astype(jnp.bfloat16)

    loop(0, hid // unit, cast_down)
    keep_down = pltpu.make_async_copy(down_own.at[member], down_all.at[pl.ds(fs * pieces, pieces)], local_sem.at[8])
    keep_down.start()


    def first_relays(i):
        e_relay(TOK, i)
        on(i + 1 < n_fs, lambda: y_relay(UV, i + 1))

    loop(0, spans, first_relays)
    loop(spans + 1, n_fs, lambda d: y_relay(UV, d))
    loop(1, n_fs, lambda d: y_relay(OUT, d))
    loop(1, n_fs, lambda d: y_ready(UV, d))

    eye = lax.broadcasted_iota(jnp.int32, (span, span), 0) == lax.broadcasted_iota(jnp.int32, (span, span), 1)
    tril = lax.broadcasted_iota(jnp.int32, (span, span), 0) >= lax.broadcasted_iota(jnp.int32, (span, span), 1)

    def mixer_span(i):
        e_finish(TOK, i)
        here = rows_at(i, span)
        square = jnp.zeros((span, 1), jnp.float32)
        for t in range(n_tp):
            wide = tok_all[t, here, :].astype(jnp.float32)
            square += jnp.sum(wide * wide, axis=-1, keepdims=True)
        inverse = lax.rsqrt(square / (n_tp * own_width) + EPS)
        pre = None
        for f in range(n_fs):
            t, sub = f // per_own, f % per_own
            wide = tok_all[t, here, sub * block:(sub + 1) * block].astype(jnp.float32)
            source = (wide * inverse * pre_gain_ref[:, f * block:(f + 1) * block]).astype(jnp.bfloat16)
            term = jnp.dot(source, uv_all[f], preferred_element_type=jnp.float32)
            pre = term if f == 0 else pre + term
        u_act = jax.nn.gelu(pre[:, :channels] * u_scale_ref[...])
        v_act = jax.nn.gelu(pre[:, channels:] * v_scale_ref[...])
        width = channels // groups
        group_of = lax.broadcasted_iota(jnp.int32, v_act.shape, 1) // width
        centre = jnp.zeros_like(v_act)
        for g in range(groups):
            mean = jnp.sum(jnp.where(group_of == g, v_act, 0.0), axis=-1, keepdims=True) / width
            centre = jnp.where(group_of == g, mean, centre)
        apart = v_act - centre
        square = apart * apart
        inverse = jnp.zeros_like(v_act)
        for g in range(groups):
            spread = jnp.sum(jnp.where(group_of == g, square, 0.0), axis=-1, keepdims=True) / width
            inverse = jnp.where(group_of == g, lax.rsqrt(spread + EPS), inverse)
        v_norm = (apart * inverse * group_gain_ref[...]).astype(jnp.bfloat16)
        mixed = jnp.zeros_like(v_act)
        for g in range(groups):
            lower = jnp.where(tril, span_ref[g].astype(jnp.float32), 0.0).astype(jnp.bfloat16)
            bias = jnp.sum(jnp.where(eye, bias_ref[g:g + 1, :], 0.0), axis=1, keepdims=True)
            term = jnp.dot(lower, v_norm, preferred_element_type=jnp.float32) + bias
            mixed = jnp.where(group_of == g, term, mixed)
        gated_all[tp, here, :] = (u_act * mixed).astype(jnp.bfloat16)
        e_push(GATED, i)

    loop(0, spans, mixer_span)
    loop(1, n_fs, lambda d: y_ready(OUT, d))
    o_each(lambda k, sub: o_copy(k, sub).start())
    for sub in range(per_own):
        out_all[tp, sub] = out_gather[tp * per_own + sub]
    loop(0, spans, lambda i: e_relay(GATED, i))

    def relay_gu(p):
        loop(1, n_fs, lambda d: y_relay(GU, d, p))

    relay_gu(0)

    o_each(o_take)

    def scale_arrived(sub):
        def take():
            for which in range(2):
                copy(out_scale_ref, scale_all.at[which, sub], s_send.at[which, 0], s_recv.at[which, sub],
                     fs=pair).wait_recv()

        on(tp * per_own + sub != fs, take)

    loop(0, per_own, scale_arrived)

    def resid_span(i):
        e_finish(GATED, i)
        here = rows_at(i, span)
        for sub in range(per_own):
            mix = None
            for s in range(n_tp):
                term = jnp.dot(gated_all[s, here, :], out_all[s, sub], preferred_element_type=jnp.float32)
                mix = term if s == 0 else mix + term
            mix = (mix * scale_all[0, sub]).astype(jnp.bfloat16)
            cols = slice(sub * block, (sub + 1) * block)
            resid_all[member, tp, here, cols] = (
                tok_all[tp, here, cols].astype(jnp.float32) + mix.astype(jnp.float32)).astype(jnp.bfloat16)
        e_push(OWN, i)
        p_copy(i, member).start()

    loop(0, spans, resid_span)
    for p in range(early_cuts, cuts):
        z_start(GU, p, p + 1)

    def norm_span(which, i):
        here = rows_at(i, span)
        square = jnp.zeros((span, 1), jnp.float32)
        for t in range(n_tp):
            wide = resid_all[which, t, here, :].astype(jnp.float32)
            square += jnp.sum(wide * wide, axis=-1, keepdims=True)
        inverse = lax.rsqrt(square / (n_tp * own_width) + EPS)
        there = rows_at(which * spans + i, span)
        for f in range(n_fs):
            t, sub = f // per_own, f % per_own
            wide = resid_all[which, t, here, sub * block:(sub + 1) * block].astype(jnp.float32)
            gain = ffn_gain_ref[:, f * block:(f + 1) * block]
            normed[f, there, :] = (wide * inverse * gain).astype(jnp.bfloat16)

    done = 1
    for i in range(spans):
        e_relay(OWN, i)
        if i % 2 and done < early_cuts - 1:
            relay_gu(done)
            done += 1

    def own_span(i):
        e_finish(OWN, i)
        norm_span(member, i)

    loop(0, spans, own_span)
    for p in range(done, early_cuts):
        relay_gu(p)

    def pair_span(i):
        p_copy(i, 1 - member).wait_recv()
        e_push(PAIR, i)

    loop(0, spans, pair_span)
    late = max(cuts - 2, early_cuts)
    for p in range(early_cuts, late):
        relay_gu(p)
    loop(0, spans, lambda i: e_relay(PAIR, i))
    for p in range(late, cuts - 1):
        relay_gu(p)

    def other_span(i):
        e_finish(PAIR, i)
        norm_span(1 - member, i)

    loop(0, spans, other_span)

    keep_gu.wait()

    loop(pieces, units, lambda k: z_copy(DN, *unit_at(k)).start())

    def first_gu(i):
        here = rows_at(i, CHUNK)
        gu_acc[here, :] = jnp.dot(normed[fs, here, :], gu_all[fs], preferred_element_type=jnp.float32)

    loop(0, chunks, first_gu)


    def fold_gu(d):
        for p in range(cuts):
            y_ready(GU, d, p)
        f = flip(fs, d, n_fs)

        def body(i):
            here = rows_at(i, CHUNK)
            gu_acc[here, :] += jnp.dot(normed[f, here, :], gu_all[f], preferred_element_type=jnp.float32)

        loop(0, chunks, body)

    relay_gu(cuts - 1)
    loop(1, n_fs - 1, fold_gu)
    loop(pieces, pieces + 1, lambda k: y_relay(DN, *unit_at(k)))
    fold_gu(jnp.int32(n_fs - 1))

    second = member == 1

    def hidden_chunk(i):
        here = rows_at(i, 64)
        tiles = main // LANES
        for j in range(tiles):
            gate_scale = jnp.where(second, gate_scale_ref[tiles + 1 + j:tiles + 2 + j], gate_scale_ref[j:j + 1])
            up_scale = jnp.where(second, up_scale_ref[tiles + 1 + j:tiles + 2 + j], up_scale_ref[j:j + 1])
            a = gu_acc[here, j * LANES:(j + 1) * LANES] * gate_scale
            b = gu_acc[here, main + j * LANES:main + (j + 1) * LANES] * up_scale
            hidden[here, j * LANES:(j + 1) * LANES] = (a / (1.0 + jnp.exp(-a)) * b).astype(jnp.bfloat16)
        gs, us = gate_scale_ref[tiles:tiles + 1], up_scale_ref[tiles:tiles + 1]
        a = gu_acc[here, 2 * main:] * jnp.where(second, jnp.where(low, swap(gs), us), jnp.where(low, gs, swap(us)))
        b = swap(a)
        last = (a / (1.0 + jnp.exp(-a)) * b).astype(jnp.bfloat16)
        hidden[here, main:hid] = last[:, 0:hid - main]

    loop(0, total_rows // 64, hidden_chunk)
    keep_down.wait()
    loop(pieces + 1, pieces + 2, lambda k: y_relay(DN, *unit_at(k)))

    def places(s):
        d, p = unit_at(s)
        b = flip(fs, d, n_fs)
        own = lax.div(b, jnp.int32(per_own))
        sub = lax.rem(b, jnp.int32(per_own)) * pieces + p
        return b * pieces + p, lax.rem(own, two), lax.div(own, two), sub, own

    def m_copy(k, j):
        b, oc, ox, sub, own = places(k)
        here = rows_at(j, CHUNK)
        return copy(part.at[b, here], mate_in.at[ox, sub, here], m_send.at[b, j], m_recv.at[ox, sub, j], tp=mate)

    def x_copy(k, j):
        b, oc, ox, sub, own = places(k)
        here = rows_at(j, CHUNK)
        d = flip(xi, ox, n_x)
        return copy(part.at[b, here], x_in.at[d - 1, sub, here], x_send.at[b, j], x_recv.at[d - 1, sub, j], tp=own)

    def q_copy(k, j):
        b, oc, ox, sub, own = places(k)
        src = part.at[b, rows_at((1 - member) * half_chunks + j, CHUNK)]
        return copy(src, pair_in.at[sub, rows_at(j, CHUNK)], q_send.at[sub, j], q_recv.at[sub, j], fs=pair)

    def down_one(k):
        b, oc, ox, sub, own = places(k)
        d, p = unit_at(k)
        on(d > 0, lambda: y_ready(DN, d, p))

        def body(j):
            here = rows_at(j, CHUNK)
            part[b, here, :] = jnp.dot(hidden[here, :], down_all[b], preferred_element_type=jnp.float32).astype(
                jnp.bfloat16)
            on(core != oc, lambda: m_copy(k, j).start())

        loop(0, chunks, body)

    def across(k):
        b, oc, ox, sub, own = places(k)

        def body(j):
            here = rows_at(j, CHUNK)
            m_copy(k, j).wait_recv()
            part[b, here, :] = (part[b, here, :].astype(jnp.float32)
                                + mate_in[ox, sub, here, :].astype(jnp.float32)).astype(jnp.bfloat16)
            on(xi != ox, lambda: x_copy(k, j).start())

        on(core == oc, lambda: loop(0, chunks, body))

    def collect(k):
        b, oc, ox, sub, own = places(k)

        def body(jj):
            j = lax.rem((1 - member) * half_chunks + jj, jnp.int32(chunks))
            here = rows_at(j, CHUNK)
            total = part[b, here, :].astype(jnp.float32)
            for dx in range(1, n_x):
                copy(part.at[b, here], x_in.at[dx - 1, sub, here], x_send.at[b, j], x_recv.at[dx - 1, sub, j],
                     tp=mate).wait_recv()
                total += x_in[dx - 1, sub, here, :].astype(jnp.float32)
            part[b, here, :] = total.astype(jnp.bfloat16)
            on(jj < half_chunks, lambda: q_copy(k, jj).start())

        on(own == tp, lambda: loop(0, chunks, body))

    def down_step(step):
        down_one(step)
        across(step)
        on(jnp.logical_and(step >= pieces - 1, step + 3 < units), lambda: y_relay(DN, *unit_at(step + 3)))

    loop(0, units, down_step)
    loop(0, units, collect)

    for sub in range(per_owner):
        b = tp * per_owner + sub
        cols = slice(sub * width_down, (sub + 1) * width_down)

        def close(j, b=b, sub=sub, cols=cols):
            here = rows_at(j, CHUNK)
            copy(part.at[b, here], pair_in.at[sub, here], q_send.at[sub, j], q_recv.at[sub, j], fs=pair).wait_recv()
            mine = rows_at(member * half_chunks + j, CHUNK)
            total = part[b, mine, :].astype(jnp.float32) + pair_in[sub, here, :].astype(jnp.float32)
            total = (total * scale_all[1, sub // pieces, :, sub % pieces * width_down:(sub % pieces + 1) * width_down]).astype(jnp.bfloat16).astype(jnp.float32)
            kept = resid_all[member, tp, here, cols].astype(jnp.float32)
            result_ref[here, cols] = (kept + total).astype(jnp.bfloat16)

        loop(0, half_chunks, close)

    for kind, count in ((UV, 1), (OUT, 1), (GU, cuts), (DN, pieces)):
        def sent(d, kind=kind, count=count):
            for p in range(count):
                z_copy(kind, d, p).wait_send()
                for e in range(1, n_rep):
                    y_copy(kind, d, e, p).wait_send()

        loop(1, n_fs, sent)

    def spans_sent(i):
        for kind in range(4):
            e_sent(kind, i)
        p_copy(i, member).wait_send()

    loop(0, spans, spans_sent)
    o_each(lambda k, sub: o_copy(k, sub).wait_send())
    s_each(lambda c: c.wait_send())

    def parts_sent(k):
        b, oc, ox, sub, own = places(k)

        def body(j):
            on(core != oc, lambda: m_copy(k, j).wait_send())
            on(jnp.logical_and(core == oc, xi != ox), lambda: x_copy(k, j).wait_send())
            on(jnp.logical_and(own == tp, j < half_chunks), lambda: q_copy(k, j).wait_send())

        loop(0, chunks, body)

    loop(0, units, parts_sent)


def shards(
    sizes,
    tokens,
    pre_gain,
    u_weight,
    u_scale,
    v_weight,
    v_scale,
    group_gain,
    span_weight,
    span_bias,
    out_weight,
    out_scale,
    ffn_gain,
    gate_weight,
    gate_scale,
    up_weight,
    up_scale,
    down_weight,
    down_scale,
):
    n_rep, n_fs, n_tp = sizes
    n_x = n_tp // 2
    extra = (LANES - gate_weight.shape[1]) % (2 * LANES)
    if extra:
        gate_weight, up_weight = (jnp.pad(w, ((0, 0), (0, extra))) for w in (gate_weight, up_weight))
        gate_scale, up_scale = (jnp.pad(s, (0, extra)) for s in (gate_scale, up_scale))
        down_weight = jnp.pad(down_weight, ((0, extra), (0, 0)))
    rows, own_width = tokens.shape
    block, local_hidden = gate_weight.shape
    hid = local_hidden // 2
    channels = u_weight.shape[1]
    per_own = own_width // block
    spans = rows // span_weight.shape[1]
    chunks = 2 * rows // CHUNK
    pieces = max(block // (2 * LANES), 1)
    width_down, per_owner, units = block // pieces, per_own * pieces, n_fs * pieces
    row = lambda vector: vector.reshape(1, -1)
    operands = (
        tokens, u_weight, v_weight, out_weight, gate_weight, up_weight, down_weight, row(out_scale), row(down_scale),
        row(pre_gain), row(ffn_gain), row(u_scale), row(v_scale), row(group_gain), span_weight, span_bias,
        gate_scale.reshape(-1, LANES), up_scale.reshape(-1, LANES),
    )
    hbm, vmem = pl.BlockSpec(memory_space=pl.ANY), pl.BlockSpec(memory_space=pltpu.VMEM)
    bf16, f32 = jnp.bfloat16, jnp.float32
    dma = lambda *shape: pltpu.SemaphoreType.DMA(shape)
    return pl.pallas_call(
        functools.partial(layer_kernel, sizes),
        out_shape=jax.ShapeDtypeStruct((rows, own_width), bf16),
        in_specs=[hbm] * 7 + [vmem] * 11,
        out_specs=vmem,
        scratch_shapes=[
            pltpu.VMEM((block, channels), f32),
            pltpu.VMEM((block, channels), f32),
            pltpu.VMEM((channels, block), f32),
            pltpu.VMEM((block, local_hidden), f32),
            pltpu.VMEM((block, local_hidden), f32),
            pltpu.VMEM((local_hidden, block), f32),
            pltpu.VMEM((2, block, 2 * hid), bf16),
            pltpu.VMEM((2, pieces, hid, width_down), bf16),
            pltpu.VMEM((n_tp, rows, own_width), bf16),
            pltpu.VMEM((n_fs, block, 2 * channels), bf16),
            pltpu.VMEM((n_fs, channels, block), bf16),
            pltpu.VMEM((n_tp, per_own, channels, block), bf16),
            pltpu.VMEM((2, per_own, 1, block), f32),
            pltpu.VMEM((n_tp, rows, channels), bf16),
            pltpu.VMEM((2, n_tp, rows, own_width), bf16),
            pltpu.VMEM((n_fs, 2 * rows, block), bf16),
            pltpu.VMEM((n_fs, block, 2 * hid), bf16),
            pltpu.VMEM((units, hid, width_down), bf16),
            pltpu.VMEM((2 * rows, 2 * hid), f32),
            pltpu.VMEM((2 * rows, hid), bf16),
            pltpu.VMEM((units, 2 * rows, width_down), bf16),
            pltpu.VMEM((n_x, per_owner, 2 * rows, width_down), bf16),
            pltpu.VMEM((n_x - 1, per_owner, 2 * rows, width_down), bf16),
            pltpu.VMEM((per_owner, rows, width_down), bf16),
            dma(9),
            dma(DN + pieces, n_fs - 1),
            dma(DN + pieces, n_fs - 1),
            dma(DN + pieces, n_fs - 1, n_rep - 1),
            dma(DN + pieces, n_fs - 1, n_rep - 1),
            dma(4, spans, n_tp - 1),
            dma(4, spans, n_tp),
            dma(spans),
            dma(spans),
            dma(n_tp - 1, per_own),
            dma(n_tp - 1, per_own),
            dma(2, n_fs - 1),
            dma(2, per_own),
            dma(units, chunks),
            dma(n_x, per_owner, chunks),
            dma(units, chunks),
            dma(n_x - 1, per_owner, chunks),
            dma(per_owner, chunks // 2),
            dma(per_owner, chunks // 2),
        ],
        compiler_params=pltpu.CompilerParams(
            collective_id=0, has_side_effects=True, vmem_limit_bytes=63 * 1024 * 1024
        ),
    )(*operands)


def solution(mesh):
    placed = (
        P(("rep", "fs"), "tp"),
        P(),
        P("fs", "tp"),
        P("tp"),
        P("fs", "tp"),
        P("tp"),
        P("tp"),
        P("tp", None, None),
        P("tp", None),
        P("tp", "fs"),
        P("fs"),
        P(),
        P("fs", "tp"),
        P("tp"),
        P("fs", "tp"),
        P("tp"),
        P("tp", "fs"),
        P("fs"),
    )
    sizes = (mesh.shape["rep"], mesh.shape["fs"], mesh.shape["tp"])
    return jax.shard_map(
        functools.partial(shards, sizes), mesh=mesh, in_specs=placed, out_specs=P(("rep", "fs"), "tp"), check_vma=False
    )
```

```python
import functools

import jax
import jax.numpy as jnp
from jax import lax
from jax.experimental import pallas as pl
from jax.experimental.pallas import tpu as pltpu
from jax.sharding import PartitionSpec as P

EPS = 0.02
MESH = pl.DeviceIdType.MESH
LANES = 128
CUTS = 8
UV, OUT, GU, DN = 0, 1, 2, 2 + CUTS
TOK, GATED, OWN, PAIR = range(4)
CHUNK = 256


def on(condition, action):
    if isinstance(condition, bool):
        if condition:
            action()
    else:
        pl.when(condition)(action)


def flip(a, d, size):
    total, bit = 0, 1
    while bit < size:
        total = total + lax.rem(lax.div(a, jnp.int32(bit)) + lax.div(jnp.int32(d), jnp.int32(bit)), jnp.int32(2)) * bit
        bit *= 2
    return total


def loop(low, high, body):
    def step(i, carry):
        body(i)
        return carry

    lax.fori_loop(low, high, step, 0)


def layer_kernel(
    sizes,
    tokens_ref,
    u_ref,
    v_ref,
    out_ref,
    gate_ref,
    up_ref,
    down_ref,
    out_scale_ref,
    down_scale_ref,
    pre_gain_ref,
    ffn_gain_ref,
    u_scale_ref,
    v_scale_ref,
    group_gain_ref,
    span_ref,
    bias_ref,
    gate_scale_ref,
    up_scale_ref,
    result_ref,
    u_f,
    v_f,
    out_f,
    gate_f,
    up_f,
    down_f,
    gu_own,
    down_own,
    tok_all,
    uv_all,
    out_gather,
    out_all,
    scale_all,
    gated_all,
    resid_all,
    normed,
    gu_all,
    down_all,
    gu_acc,
    hidden,
    part,
    mate_in,
    x_in,
    pair_in,
    local_sem,
    z_send,
    z_recv,
    y_send,
    y_recv,
    e_send,
    e_recv,
    p_send,
    p_recv,
    o_send,
    o_recv,
    s_send,
    s_recv,
    m_send,
    m_recv,
    x_send,
    x_recv,
    q_send,
    q_recv,
):
    n_rep, n_fs, n_tp = sizes
    n_x = n_tp // 2
    rows, own_width = tokens_ref.shape
    block = gate_ref.shape[0]
    per_own = own_width // block
    hid = gate_ref.shape[1] // 2
    cuts = min(CUTS, block // n_rep // 16)
    early_cuts = cuts // 2
    pieces, width_down = down_own.shape[1], down_own.shape[3]
    per_owner = per_own * pieces
    units = n_fs * pieces
    main = hid // LANES * LANES
    channels = u_ref.shape[1]
    groups, span = span_ref.shape[0], span_ref.shape[1]
    spans = rows // span
    total_rows = 2 * rows
    chunks = total_rows // CHUNK
    half_chunks = chunks // 2
    rep, fs, tp = lax.axis_index("rep"), lax.axis_index("fs"), lax.axis_index("tp")
    two = jnp.int32(2)
    member = lax.rem(fs, two)
    core, xi = lax.rem(tp, two), lax.div(tp, two)
    mate = tp + 1 - 2 * core
    pair = fs + 1 - 2 * member
    owner = lax.div(fs, jnp.int32(per_own))
    owner_sub = lax.rem(fs, jnp.int32(per_own))

    def copy(src, dst, send_sem, recv_sem, **device):
        return pltpu.make_async_remote_copy(
            src_ref=src, dst_ref=dst, send_sem=send_sem, recv_sem=recv_sem, device_id=device, device_id_type=MESH)

    def rows_at(i, size):
        return pl.ds(pl.multiple_of(i * size, size), size)

    def w_rows(kind, r, p=0):
        if kind == GU:
            size = block // n_rep // cuts
            return pl.ds(pl.multiple_of((cuts * r + p) * size, size), size)
        size = (block if kind == UV else channels if kind == OUT else hid) // n_rep
        return pl.ds(pl.multiple_of(r * size, size), size)

    def w_slot(kind, f, r, p=0):
        if kind == DN:
            return down_all.at[f * pieces + p, w_rows(kind, r)]
        ref = uv_all if kind == UV else out_gather if kind == OUT else gu_all
        return ref.at[f, w_rows(kind, r, p)]

    def w_source(kind, g, p=0):
        if kind in (UV, OUT):
            return w_slot(kind, fs, rep)
        if kind == DN:
            return down_own.at[lax.rem(g, two), p, w_rows(kind, rep)]
        return gu_own.at[lax.rem(g, two), w_rows(kind, rep, p)]

    def z_pass(kind):
        slot = w_slot(kind, flip(fs, 2, n_fs), rep)
        return copy(slot, slot, z_send.at[kind, 2], z_recv.at[kind, 2], fs=pair)

    def z_copy(kind, d, p=0):
        g = flip(fs, d, n_fs)
        return copy(w_source(kind, g, p), w_slot(kind, fs, rep, p), z_send.at[kind + p, d - 1],
                    z_recv.at[kind + p, d - 1], fs=g)

    def y_copy(kind, d, e, p=0):
        slot = w_slot(kind, flip(fs, d, n_fs), rep, p)
        return copy(slot, slot, y_send.at[kind + p, d - 1, e - 1], y_recv.at[kind + p, d - 1, e - 1],
                    rep=lax.rem(rep + e, jnp.int32(n_rep)))

    def z_start(kind, low=0, high=1):
        def body(d):
            for p in range(low, high):
                on(d != 3 if kind in (UV, OUT) else True, lambda: z_copy(kind, d, p).start())

        loop(1, n_fs, body)

    def unit_at(k):
        k = jnp.int32(k)
        return lax.div(k, jnp.int32(pieces)), lax.rem(k, jnp.int32(pieces))

    def y_relay(kind, d, p=0):
        slot = w_slot(kind, flip(fs, d, n_fs), rep, p)
        copy(slot, slot, z_send.at[kind + p, d - 1], z_recv.at[kind + p, d - 1], fs=pair).wait_recv()
        if kind in (UV, OUT):
            on(d == 2, lambda: z_pass(kind).start())
        for e in range(1, n_rep):
            y_copy(kind, d, e, p).start()

    def y_ready(kind, d, p=0):
        for e in range(1, n_rep):
            slot = w_slot(kind, flip(fs, d, n_fs), lax.rem(rep - e + n_rep, jnp.int32(n_rep)), p)
            copy(slot, slot, y_send.at[kind + p, d - 1, e - 1], y_recv.at[kind + p, d - 1, e - 1],
                 rep=lax.rem(rep + 1, jnp.int32(n_rep))).wait_recv()

    def e_slot(kind, i, t):
        here = rows_at(i, span)
        if kind == TOK:
            return tok_all.at[t, here]
        if kind == GATED:
            return gated_all.at[t, here]
        return resid_all.at[member if kind == OWN else 1 - member, t, here]

    def x_peer(dx):
        return 2 * flip(xi, dx, n_x) + core

    def e_copy(kind, i, t, k, to):
        slot = e_slot(kind, i, t)
        return copy(slot, slot, e_send.at[kind, i, k], e_recv.at[kind, i, t], tp=to)

    def e_list(kind, i):
        out = [e_copy(kind, i, tp, 0, mate)]
        for dx in range(1, n_x):
            out.append(e_copy(kind, i, tp, dx, x_peer(dx)))
        return out

    def e_push(kind, i):
        for c in e_list(kind, i):
            c.start()

    def e_wait(kind, i, t):
        e_copy(kind, i, t, 0, mate).wait_recv()

    def e_relay(kind, i):
        for dx in range(1, n_x):
            e_wait(kind, i, x_peer(dx))
            e_copy(kind, i, x_peer(dx), n_x - 1 + dx, mate).start()

    def e_finish(kind, i):
        for dx in range(n_x):
            e_wait(kind, i, 2 * flip(xi, dx, n_x) + 1 - core)

    def e_sent(kind, i):
        for c in e_list(kind, i):
            c.wait_send()
        for dx in range(1, n_x):
            e_copy(kind, i, x_peer(dx), n_x - 1 + dx, mate).wait_send()

    def p_copy(i, which):
        slot = resid_all.at[which, tp, rows_at(i, span)]
        return copy(slot, slot, p_send.at[i], p_recv.at[i], fs=pair)

    def o_copy(k, sub):
        to = lax.rem(tp + k, jnp.int32(n_tp))
        return copy(out_gather.at[to * per_own + sub], out_all.at[tp, sub], o_send.at[k - 1, sub],
                    o_recv.at[k - 1, sub], tp=to)

    def o_take(k, sub):
        sender = lax.rem(tp - k + n_tp, jnp.int32(n_tp))
        copy(out_gather.at[0], out_all.at[sender, sub], o_send.at[k - 1, sub], o_recv.at[k - 1, sub],
             tp=mate).wait_recv()

    def o_each(action):
        for k in range(1, n_tp):
            for sub in range(per_own):
                action(k, sub)

    def s_copy(d, which):
        g = flip(fs, d, n_fs)
        src = (out_scale_ref, down_scale_ref)[which]
        return copy(src, scale_all.at[which, owner_sub], s_send.at[which, d - 1], s_recv.at[which, owner_sub], fs=g)

    loads = [
        pltpu.make_async_copy(src, dst, local_sem.at[i])
        for i, (src, dst) in enumerate((
            (tokens_ref, tok_all.at[tp]), (u_ref, u_f), (v_ref, v_f), (out_ref, out_f), (gate_ref, gate_f),
            (up_ref, up_f), (down_ref, down_f)))
    ]
    for load in loads:
        load.start()

    barrier = pltpu.get_barrier_semaphore()

    def greet(**device):
        pl.semaphore_signal(barrier, inc=1, device_id=device, device_id_type=MESH)

    for k in range(1, n_tp):
        greet(tp=lax.rem(tp + k, jnp.int32(n_tp)))
    loop(1, n_fs, lambda d: greet(fs=flip(fs, d, n_fs)))
    for e in range(1, n_rep):
        greet(rep=lax.rem(rep + e, jnp.int32(n_rep)))
    pl.semaphore_wait(barrier, n_tp + n_fs + n_rep - 3)

    loads[0].wait()
    loop(0, spans, lambda i: e_push(TOK, i))
    loads[1].wait()
    loads[2].wait()
    uv_all[fs, :, 0:channels] = u_f[...].astype(jnp.bfloat16)
    uv_all[fs, :, channels:2 * channels] = v_f[...].astype(jnp.bfloat16)
    z_start(UV)
    loads[3].wait()
    out_gather[fs] = out_f[...].astype(jnp.bfloat16)
    z_start(OUT)

    def keep_own():
        scale_all[0, owner_sub] = out_scale_ref[...]
        scale_all[1, owner_sub] = down_scale_ref[...]

    on(owner == tp, keep_own)

    def s_each(action):
        def body(d):
            for which in range(2):
                action(s_copy(d, which))

        on(owner == tp, lambda: loop(1, n_fs, body))

    s_each(lambda c: c.start())

    low = lax.broadcasted_iota(jnp.int32, (1, LANES), 1) < LANES // 2
    unit = 64

    def swap(value):
        return pltpu.roll(value, LANES // 2, 1)

    loads[4].wait()
    loads[5].wait()

    def cast_gu(i):
        here = rows_at(i, unit)
        for member_of in range(2):
            first = member_of * (main + LANES)
            gu_own[member_of, here, 0:main] = gate_f[here, first:first + main].astype(jnp.bfloat16)
            gu_own[member_of, here, main:2 * main] = up_f[here, first:first + main].astype(jnp.bfloat16)
        g, u = gate_f[here, main:main + LANES], up_f[here, main:main + LANES]
        gu_own[0, here, 2 * main:] = jnp.where(low, g, swap(u)).astype(jnp.bfloat16)
        gu_own[1, here, 2 * main:] = jnp.where(low, swap(g), u).astype(jnp.bfloat16)

    loop(0, block // unit, cast_gu)
    z_start(GU, 0, 1)
    keep_gu = pltpu.make_async_copy(gu_own.at[member], gu_all.at[fs], local_sem.at[7])
    keep_gu.start()
    loads[6].wait()

    def cast_down(i):
        here = rows_at(i, unit)
        there = rows_at(jnp.where(i < main // unit, i + (main + LANES) // unit, main // unit + 1), unit)
        for p in range(pieces):
            cols = slice(p * width_down, (p + 1) * width_down)
            down_own[0, p, here] = down_f[here, cols].astype(jnp.bfloat16)
            down_own[1, p, here] = down_f[there, cols].astype(jnp.bfloat16)

    loop(0, hid // unit, cast_down)
    keep_down = pltpu.make_async_copy(down_own.at[member], down_all.at[pl.ds(fs * pieces, pieces)], local_sem.at[8])
    keep_down.start()


    def first_relays(i):
        e_relay(TOK, i)
        on(i + 1 < n_fs, lambda: y_relay(UV, i + 1))

    loop(0, spans, first_relays)
    loop(spans + 1, n_fs, lambda d: y_relay(UV, d))
    loop(1, n_fs, lambda d: y_relay(OUT, d))
    for p in range(1, early_cuts):
        z_start(GU, p, p + 1)
    loop(1, n_fs, lambda d: y_ready(UV, d))

    eye = lax.broadcasted_iota(jnp.int32, (span, span), 0) == lax.broadcasted_iota(jnp.int32, (span, span), 1)
    tril = lax.broadcasted_iota(jnp.int32, (span, span), 0) >= lax.broadcasted_iota(jnp.int32, (span, span), 1)

    def mixer_span(i):
        e_finish(TOK, i)
        here = rows_at(i, span)
        square = jnp.zeros((span, 1), jnp.float32)
        for t in range(n_tp):
            wide = tok_all[t, here, :].astype(jnp.float32)
            square += jnp.sum(wide * wide, axis=-1, keepdims=True)
        inverse = lax.rsqrt(square / (n_tp * own_width) + EPS)
        pre = None
        for f in range(n_fs):
            t, sub = f // per_own, f % per_own
            wide = tok_all[t, here, sub * block:(sub + 1) * block].astype(jnp.float32)
            source = (wide * inverse * pre_gain_ref[:, f * block:(f + 1) * block]).astype(jnp.bfloat16)
            term = jnp.dot(source, uv_all[f], preferred_element_type=jnp.float32)
            pre = term if f == 0 else pre + term
        u_act = jax.nn.gelu(pre[:, :channels] * u_scale_ref[...])
        v_act = jax.nn.gelu(pre[:, channels:] * v_scale_ref[...])
        width = channels // groups
        group_of = lax.broadcasted_iota(jnp.int32, v_act.shape, 1) // width
        centre = jnp.zeros_like(v_act)
        for g in range(groups):
            mean = jnp.sum(jnp.where(group_of == g, v_act, 0.0), axis=-1, keepdims=True) / width
            centre = jnp.where(group_of == g, mean, centre)
        apart = v_act - centre
        square = apart * apart
        inverse = jnp.zeros_like(v_act)
        for g in range(groups):
            spread = jnp.sum(jnp.where(group_of == g, square, 0.0), axis=-1, keepdims=True) / width
            inverse = jnp.where(group_of == g, lax.rsqrt(spread + EPS), inverse)
        v_norm = (apart * inverse * group_gain_ref[...]).astype(jnp.bfloat16)
        mixed = jnp.zeros_like(v_act)
        for g in range(groups):
            lower = jnp.where(tril, span_ref[g].astype(jnp.float32), 0.0).astype(jnp.bfloat16)
            bias = jnp.sum(jnp.where(eye, bias_ref[g:g + 1, :], 0.0), axis=1, keepdims=True)
            term = jnp.dot(lower, v_norm, preferred_element_type=jnp.float32) + bias
            mixed = jnp.where(group_of == g, term, mixed)
        gated_all[tp, here, :] = (u_act * mixed).astype(jnp.bfloat16)
        e_push(GATED, i)

    loop(0, spans, mixer_span)
    loop(1, n_fs, lambda d: y_ready(OUT, d))
    o_each(lambda k, sub: o_copy(k, sub).start())
    for sub in range(per_own):
        out_all[tp, sub] = out_gather[tp * per_own + sub]
    loop(0, spans, lambda i: e_relay(GATED, i))

    def relay_gu(p):
        loop(1, n_fs, lambda d: y_relay(GU, d, p))

    relay_gu(0)

    o_each(o_take)

    def scale_arrived(sub):
        def take():
            for which in range(2):
                copy(out_scale_ref, scale_all.at[which, sub], s_send.at[which, 0], s_recv.at[which, sub],
                     fs=pair).wait_recv()

        on(tp * per_own + sub != fs, take)

    loop(0, per_own, scale_arrived)

    def resid_span(i):
        e_finish(GATED, i)
        here = rows_at(i, span)
        for sub in range(per_own):
            mix = None
            for s in range(n_tp):
                term = jnp.dot(gated_all[s, here, :], out_all[s, sub], preferred_element_type=jnp.float32)
                mix = term if s == 0 else mix + term
            mix = (mix * scale_all[0, sub]).astype(jnp.bfloat16)
            cols = slice(sub * block, (sub + 1) * block)
            resid_all[member, tp, here, cols] = (
                tok_all[tp, here, cols].astype(jnp.float32) + mix.astype(jnp.float32)).astype(jnp.bfloat16)
        e_push(OWN, i)
        p_copy(i, member).start()

    loop(0, spans, resid_span)
    for p in range(early_cuts, cuts):
        z_start(GU, p, p + 1)

    def norm_span(which, i):
        here = rows_at(i, span)
        square = jnp.zeros((span, 1), jnp.float32)
        for t in range(n_tp):
            wide = resid_all[which, t, here, :].astype(jnp.float32)
            square += jnp.sum(wide * wide, axis=-1, keepdims=True)
        inverse = lax.rsqrt(square / (n_tp * own_width) + EPS)
        there = rows_at(which * spans + i, span)
        for f in range(n_fs):
            t, sub = f // per_own, f % per_own
            wide = resid_all[which, t, here, sub * block:(sub + 1) * block].astype(jnp.float32)
            gain = ffn_gain_ref[:, f * block:(f + 1) * block]
            normed[f, there, :] = (wide * inverse * gain).astype(jnp.bfloat16)

    done = 1
    for i in range(spans):
        e_relay(OWN, i)
        if done < early_cuts:
            relay_gu(done)
            done += 1

    def own_span(i):
        e_finish(OWN, i)
        norm_span(member, i)

    loop(0, spans, own_span)
    for p in range(done, early_cuts):
        relay_gu(p)

    outer = jnp.logical_or(fs == 0, fs == n_fs - 1)
    late = max(cuts - 2, early_cuts)

    def relay_some(low, high):
        for p in range(early_cuts, late - 1):
            loop(low, high, lambda d: y_relay(GU, d, p))

    on(outer, lambda: relay_some(2, n_fs))

    def pair_span(i):
        p_copy(i, 1 - member).wait_recv()
        e_push(PAIR, i)

    loop(0, spans, pair_span)
    relay_some(1, jnp.where(outer, 2, n_fs))
    for p in range(late - 1, late):
        loop(2, n_fs, lambda d: y_relay(GU, d, p))
        y_relay(GU, 1, p)
    loop(0, spans // 2, lambda i: e_relay(PAIR, i))
    for p in range(late, cuts - 1):
        relay_gu(p)
    loop(spans // 2, spans, lambda i: e_relay(PAIR, i))

    def other_span(i):
        e_finish(PAIR, i)
        norm_span(1 - member, i)

    loop(0, spans, other_span)

    keep_gu.wait()

    loop(pieces, units, lambda k: z_copy(DN, *unit_at(k)).start())

    def first_gu(i):
        here = rows_at(i, CHUNK)
        gu_acc[here, :] = jnp.dot(normed[fs, here, :], gu_all[fs], preferred_element_type=jnp.float32)

    loop(0, chunks, first_gu)


    def fold_gu(d):
        for p in range(cuts):
            y_ready(GU, d, p)
        f = flip(fs, d, n_fs)

        def body(i):
            here = rows_at(i, CHUNK)
            gu_acc[here, :] += jnp.dot(normed[f, here, :], gu_all[f], preferred_element_type=jnp.float32)

        loop(0, chunks, body)

    relay_gu(cuts - 1)
    loop(1, n_fs - 1, fold_gu)
    loop(pieces, pieces + 1, lambda k: y_relay(DN, *unit_at(k)))
    fold_gu(jnp.int32(n_fs - 1))

    second = member == 1

    def hidden_chunk(i):
        here = rows_at(i, 64)
        tiles = main // LANES
        for j in range(tiles):
            gate_scale = jnp.where(second, gate_scale_ref[tiles + 1 + j:tiles + 2 + j], gate_scale_ref[j:j + 1])
            up_scale = jnp.where(second, up_scale_ref[tiles + 1 + j:tiles + 2 + j], up_scale_ref[j:j + 1])
            a = gu_acc[here, j * LANES:(j + 1) * LANES] * gate_scale
            b = gu_acc[here, main + j * LANES:main + (j + 1) * LANES] * up_scale
            hidden[here, j * LANES:(j + 1) * LANES] = (a / (1.0 + jnp.exp(-a)) * b).astype(jnp.bfloat16)
        gs, us = gate_scale_ref[tiles:tiles + 1], up_scale_ref[tiles:tiles + 1]
        a = gu_acc[here, 2 * main:] * jnp.where(second, jnp.where(low, swap(gs), us), jnp.where(low, gs, swap(us)))
        b = swap(a)
        last = (a / (1.0 + jnp.exp(-a)) * b).astype(jnp.bfloat16)
        hidden[here, main:hid] = last[:, 0:hid - main]

    loop(0, total_rows // 64, hidden_chunk)
    keep_down.wait()
    loop(pieces + 1, 2 * pieces + 1, lambda k: y_relay(DN, *unit_at(k)))

    def places(s):
        d, p = unit_at(s)
        b = flip(fs, d, n_fs)
        own = lax.div(b, jnp.int32(per_own))
        sub = lax.rem(b, jnp.int32(per_own)) * pieces + p
        return b * pieces + p, lax.rem(own, two), lax.div(own, two), sub, own

    def m_copy(k, j):
        b, oc, ox, sub, own = places(k)
        here = rows_at(j, CHUNK)
        return copy(part.at[b, here], mate_in.at[ox, sub, here], m_send.at[b, j], m_recv.at[ox, sub, j], tp=mate)

    def x_copy(k, j):
        b, oc, ox, sub, own = places(k)
        here = rows_at(j, CHUNK)
        d = flip(xi, ox, n_x)
        return copy(part.at[b, here], x_in.at[d - 1, sub, here], x_send.at[b, j], x_recv.at[d - 1, sub, j], tp=own)

    def q_copy(k, j):
        b, oc, ox, sub, own = places(k)
        src = part.at[b, rows_at((1 - member) * half_chunks + j, CHUNK)]
        return copy(src, pair_in.at[sub, rows_at(j, CHUNK)], q_send.at[sub, j], q_recv.at[sub, j], fs=pair)

    def down_one(k):
        b, oc, ox, sub, own = places(k)
        d, p = unit_at(k)
        on(d > 0, lambda: y_ready(DN, d, p))

        def body(j):
            here = rows_at(j, CHUNK)
            part[b, here, :] = jnp.dot(hidden[here, :], down_all[b], preferred_element_type=jnp.float32).astype(
                jnp.bfloat16)
            on(core != oc, lambda: m_copy(k, j).start())

        loop(0, chunks, body)

    def across(k):
        b, oc, ox, sub, own = places(k)

        def body(j):
            here = rows_at(j, CHUNK)
            m_copy(k, j).wait_recv()
            part[b, here, :] = (part[b, here, :].astype(jnp.float32)
                                + mate_in[ox, sub, here, :].astype(jnp.float32)).astype(jnp.bfloat16)
            on(xi != ox, lambda: x_copy(k, j).start())

        on(core == oc, lambda: loop(0, chunks, body))

    def collect(k):
        b, oc, ox, sub, own = places(k)

        def body(jj):
            j = lax.rem((1 - member) * half_chunks + jj, jnp.int32(chunks))
            here = rows_at(j, CHUNK)
            total = part[b, here, :].astype(jnp.float32)
            for dx in range(1, n_x):
                copy(part.at[b, here], x_in.at[dx - 1, sub, here], x_send.at[b, j], x_recv.at[dx - 1, sub, j],
                     tp=mate).wait_recv()
                total += x_in[dx - 1, sub, here, :].astype(jnp.float32)
            part[b, here, :] = total.astype(jnp.bfloat16)
            on(jj < half_chunks, lambda: q_copy(k, jj).start())

        on(own == tp, lambda: loop(0, chunks, body))

    def down_step(step):
        down_one(step)
        across(step)
        on(jnp.logical_and(step >= 2 * pieces - 1, step + 2 < units), lambda: y_relay(DN, *unit_at(step + 2)))

    loop(0, units, down_step)
    loop(0, units, collect)

    for sub in range(per_owner):
        b = tp * per_owner + sub
        cols = slice(sub * width_down, (sub + 1) * width_down)

        def close(j, b=b, sub=sub, cols=cols):
            here = rows_at(j, CHUNK)
            copy(part.at[b, here], pair_in.at[sub, here], q_send.at[sub, j], q_recv.at[sub, j], fs=pair).wait_recv()
            mine = rows_at(member * half_chunks + j, CHUNK)
            total = part[b, mine, :].astype(jnp.float32) + pair_in[sub, here, :].astype(jnp.float32)
            total = (total * scale_all[1, sub // pieces, :, sub % pieces * width_down:(sub % pieces + 1) * width_down]).astype(jnp.bfloat16).astype(jnp.float32)
            kept = resid_all[member, tp, here, cols].astype(jnp.float32)
            result_ref[here, cols] = (kept + total).astype(jnp.bfloat16)

        loop(0, half_chunks, close)

    for kind, count in ((UV, 1), (OUT, 1), (GU, cuts), (DN, pieces)):
        def sent(d, kind=kind, count=count):
            for p in range(count):
                if kind in (UV, OUT):
                    on(d == 3, lambda: z_pass(kind).wait_send())
                    on(d != 3, lambda: z_copy(kind, d, p).wait_send())
                else:
                    z_copy(kind, d, p).wait_send()
                for e in range(1, n_rep):
                    y_copy(kind, d, e, p).wait_send()

        loop(1, n_fs, sent)

    def spans_sent(i):
        for kind in range(4):
            e_sent(kind, i)
        p_copy(i, member).wait_send()

    loop(0, spans, spans_sent)
    o_each(lambda k, sub: o_copy(k, sub).wait_send())
    s_each(lambda c: c.wait_send())

    def parts_sent(k):
        b, oc, ox, sub, own = places(k)

        def body(j):
            on(core != oc, lambda: m_copy(k, j).wait_send())
            on(jnp.logical_and(core == oc, xi != ox), lambda: x_copy(k, j).wait_send())
            on(jnp.logical_and(own == tp, j < half_chunks), lambda: q_copy(k, j).wait_send())

        loop(0, chunks, body)

    loop(0, units, parts_sent)


def shards(
    sizes,
    tokens,
    pre_gain,
    u_weight,
    u_scale,
    v_weight,
    v_scale,
    group_gain,
    span_weight,
    span_bias,
    out_weight,
    out_scale,
    ffn_gain,
    gate_weight,
    gate_scale,
    up_weight,
    up_scale,
    down_weight,
    down_scale,
):
    n_rep, n_fs, n_tp = sizes
    n_x = n_tp // 2
    extra = (LANES - gate_weight.shape[1]) % (2 * LANES)
    if extra:
        gate_weight, up_weight = (jnp.pad(w, ((0, 0), (0, extra))) for w in (gate_weight, up_weight))
        gate_scale, up_scale = (jnp.pad(s, (0, extra)) for s in (gate_scale, up_scale))
        down_weight = jnp.pad(down_weight, ((0, extra), (0, 0)))
    rows, own_width = tokens.shape
    block, local_hidden = gate_weight.shape
    hid = local_hidden // 2
    channels = u_weight.shape[1]
    per_own = own_width // block
    spans = rows // span_weight.shape[1]
    chunks = 2 * rows // CHUNK
    pieces = max(block // (2 * LANES), 1)
    width_down, per_owner, units = block // pieces, per_own * pieces, n_fs * pieces
    row = lambda vector: vector.reshape(1, -1)
    operands = (
        tokens, u_weight, v_weight, out_weight, gate_weight, up_weight, down_weight, row(out_scale), row(down_scale),
        row(pre_gain), row(ffn_gain), row(u_scale), row(v_scale), row(group_gain), span_weight, span_bias,
        gate_scale.reshape(-1, LANES), up_scale.reshape(-1, LANES),
    )
    hbm, vmem = pl.BlockSpec(memory_space=pl.ANY), pl.BlockSpec(memory_space=pltpu.VMEM)
    bf16, f32 = jnp.bfloat16, jnp.float32
    dma = lambda *shape: pltpu.SemaphoreType.DMA(shape)
    return pl.pallas_call(
        functools.partial(layer_kernel, sizes),
        out_shape=jax.ShapeDtypeStruct((rows, own_width), bf16),
        in_specs=[hbm] * 7 + [vmem] * 11,
        out_specs=vmem,
        scratch_shapes=[
            pltpu.VMEM((block, channels), f32),
            pltpu.VMEM((block, channels), f32),
            pltpu.VMEM((channels, block), f32),
            pltpu.VMEM((block, local_hidden), f32),
            pltpu.VMEM((block, local_hidden), f32),
            pltpu.VMEM((local_hidden, block), f32),
            pltpu.VMEM((2, block, 2 * hid), bf16),
            pltpu.VMEM((2, pieces, hid, width_down), bf16),
            pltpu.VMEM((n_tp, rows, own_width), bf16),
            pltpu.VMEM((n_fs, block, 2 * channels), bf16),
            pltpu.VMEM((n_fs, channels, block), bf16),
            pltpu.VMEM((n_tp, per_own, channels, block), bf16),
            pltpu.VMEM((2, per_own, 1, block), f32),
            pltpu.VMEM((n_tp, rows, channels), bf16),
            pltpu.VMEM((2, n_tp, rows, own_width), bf16),
            pltpu.VMEM((n_fs, 2 * rows, block), bf16),
            pltpu.VMEM((n_fs, block, 2 * hid), bf16),
            pltpu.VMEM((units, hid, width_down), bf16),
            pltpu.VMEM((2 * rows, 2 * hid), f32),
            pltpu.VMEM((2 * rows, hid), bf16),
            pltpu.VMEM((units, 2 * rows, width_down), bf16),
            pltpu.VMEM((n_x, per_owner, 2 * rows, width_down), bf16),
            pltpu.VMEM((n_x - 1, per_owner, 2 * rows, width_down), bf16),
            pltpu.VMEM((per_owner, rows, width_down), bf16),
            dma(9),
            dma(DN + pieces, n_fs - 1),
            dma(DN + pieces, n_fs - 1),
            dma(DN + pieces, n_fs - 1, n_rep - 1),
            dma(DN + pieces, n_fs - 1, n_rep - 1),
            dma(4, spans, n_tp - 1),
            dma(4, spans, n_tp),
            dma(spans),
            dma(spans),
            dma(n_tp - 1, per_own),
            dma(n_tp - 1, per_own),
            dma(2, n_fs - 1),
            dma(2, per_own),
            dma(units, chunks),
            dma(n_x, per_owner, chunks),
            dma(units, chunks),
            dma(n_x - 1, per_owner, chunks),
            dma(per_owner, chunks // 2),
            dma(per_owner, chunks // 2),
        ],
        compiler_params=pltpu.CompilerParams(
            collective_id=0, has_side_effects=True, vmem_limit_bytes=63 * 1024 * 1024
        ),
    )(*operands)


def solution(mesh):
    placed = (
        P(("rep", "fs"), "tp"),
        P(),
        P("fs", "tp"),
        P("tp"),
        P("fs", "tp"),
        P("tp"),
        P("tp"),
        P("tp", None, None),
        P("tp", None),
        P("tp", "fs"),
        P("fs"),
        P(),
        P("fs", "tp"),
        P("tp"),
        P("fs", "tp"),
        P("tp"),
        P("tp", "fs"),
        P("fs"),
    )
    sizes = (mesh.shape["rep"], mesh.shape["fs"], mesh.shape["tp"])
    return jax.shard_map(
        functools.partial(shards, sizes), mesh=mesh, in_specs=placed, out_specs=P(("rep", "fs"), "tp"), check_vma=False
    )
```

```python
import functools

import jax
import jax.numpy as jnp
from jax import lax
from jax.experimental import pallas as pl
from jax.experimental.pallas import tpu as pltpu
from jax.sharding import PartitionSpec as P

EPS = 0.02
MESH = pl.DeviceIdType.MESH
LANES = 128
CUTS = 8
UV, OUT, GU, DN = 0, 1, 2, 2 + CUTS
TOK, GATED, OWN, PAIR = range(4)
CHUNK = 256


def on(condition, action):
    if isinstance(condition, bool):
        if condition:
            action()
    else:
        pl.when(condition)(action)


def flip(a, d, size):
    total, bit = 0, 1
    while bit < size:
        total = total + lax.rem(lax.div(a, jnp.int32(bit)) + lax.div(jnp.int32(d), jnp.int32(bit)), jnp.int32(2)) * bit
        bit *= 2
    return total


def loop(low, high, body):
    def step(i, carry):
        body(i)
        return carry

    lax.fori_loop(low, high, step, 0)


def layer_kernel(
    sizes,
    tokens_ref,
    u_ref,
    v_ref,
    out_ref,
    gate_ref,
    up_ref,
    down_ref,
    out_scale_ref,
    down_scale_ref,
    pre_gain_ref,
    ffn_gain_ref,
    u_scale_ref,
    v_scale_ref,
    group_gain_ref,
    span_ref,
    bias_ref,
    gate_scale_ref,
    up_scale_ref,
    result_ref,
    u_f,
    v_f,
    out_f,
    gate_f,
    up_f,
    down_f,
    gu_own,
    down_own,
    tok_all,
    uv_all,
    out_gather,
    out_all,
    scale_all,
    gated_all,
    resid_all,
    normed,
    gu_all,
    down_all,
    gu_acc,
    hidden,
    part,
    mate_in,
    x_in,
    pair_in,
    local_sem,
    z_send,
    z_recv,
    y_send,
    y_recv,
    e_send,
    e_recv,
    p_send,
    p_recv,
    o_send,
    o_recv,
    s_send,
    s_recv,
    m_send,
    m_recv,
    x_send,
    x_recv,
    q_send,
    q_recv,
):
    n_rep, n_fs, n_tp = sizes
    n_x = n_tp // 2
    rows, own_width = tokens_ref.shape
    block = gate_ref.shape[0]
    per_own = own_width // block
    hid = gate_ref.shape[1] // 2
    cuts = min(CUTS, block // n_rep // 16)
    early_cuts = cuts // 2
    pieces, width_down = down_own.shape[1], down_own.shape[3]
    per_owner = per_own * pieces
    units = n_fs * pieces
    main = hid // LANES * LANES
    channels = u_ref.shape[1]
    groups, span = span_ref.shape[0], span_ref.shape[1]
    spans = rows // span
    total_rows = 2 * rows
    chunks = total_rows // CHUNK
    half_chunks = chunks // 2
    rep, fs, tp = lax.axis_index("rep"), lax.axis_index("fs"), lax.axis_index("tp")
    two = jnp.int32(2)
    member = lax.rem(fs, two)
    core, xi = lax.rem(tp, two), lax.div(tp, two)
    mate = tp + 1 - 2 * core
    pair = fs + 1 - 2 * member
    owner = lax.div(fs, jnp.int32(per_own))
    owner_sub = lax.rem(fs, jnp.int32(per_own))

    def copy(src, dst, send_sem, recv_sem, **device):
        return pltpu.make_async_remote_copy(
            src_ref=src, dst_ref=dst, send_sem=send_sem, recv_sem=recv_sem, device_id=device, device_id_type=MESH)

    def rows_at(i, size):
        return pl.ds(pl.multiple_of(i * size, size), size)

    def w_rows(kind, r, p=0):
        if kind == GU:
            size = block // n_rep // cuts
            return pl.ds(pl.multiple_of((cuts * r + p) * size, size), size)
        size = (block if kind == UV else channels if kind == OUT else hid) // n_rep
        return pl.ds(pl.multiple_of(r * size, size), size)

    def w_slot(kind, f, r, p=0):
        if kind == DN:
            return down_all.at[f * pieces + p, w_rows(kind, r)]
        ref = uv_all if kind == UV else out_gather if kind == OUT else gu_all
        return ref.at[f, w_rows(kind, r, p)]

    def w_source(kind, g, p=0):
        if kind in (UV, OUT):
            return w_slot(kind, fs, rep)
        if kind == DN:
            return down_own.at[lax.rem(g, two), p, w_rows(kind, rep)]
        return gu_own.at[lax.rem(g, two), w_rows(kind, rep, p)]

    def z_pass(kind):
        slot = w_slot(kind, flip(fs, 2, n_fs), rep)
        return copy(slot, slot, z_send.at[kind, 2], z_recv.at[kind, 2], fs=pair)

    def z_copy(kind, d, p=0):
        g = flip(fs, d, n_fs)
        return copy(w_source(kind, g, p), w_slot(kind, fs, rep, p), z_send.at[kind + p, d - 1],
                    z_recv.at[kind + p, d - 1], fs=g)

    def y_copy(kind, d, e, p=0):
        slot = w_slot(kind, flip(fs, d, n_fs), rep, p)
        return copy(slot, slot, y_send.at[kind + p, d - 1, e - 1], y_recv.at[kind + p, d - 1, e - 1],
                    rep=lax.rem(rep + e, jnp.int32(n_rep)))

    def z_start(kind, low=0, high=1):
        def body(d):
            for p in range(low, high):
                on(d != 3 if kind in (UV, OUT) else True, lambda: z_copy(kind, d, p).start())

        loop(1, n_fs, body)

    def unit_at(k):
        k = jnp.int32(k)
        return lax.div(k, jnp.int32(pieces)), lax.rem(k, jnp.int32(pieces))

    def y_relay(kind, d, p=0):
        slot = w_slot(kind, flip(fs, d, n_fs), rep, p)
        copy(slot, slot, z_send.at[kind + p, d - 1], z_recv.at[kind + p, d - 1], fs=pair).wait_recv()
        if kind in (UV, OUT):
            on(d == 2, lambda: z_pass(kind).start())
        for e in range(1, n_rep):
            y_copy(kind, d, e, p).start()

    def y_ready(kind, d, p=0):
        for e in range(1, n_rep):
            slot = w_slot(kind, flip(fs, d, n_fs), lax.rem(rep - e + n_rep, jnp.int32(n_rep)), p)
            copy(slot, slot, y_send.at[kind + p, d - 1, e - 1], y_recv.at[kind + p, d - 1, e - 1],
                 rep=lax.rem(rep + 1, jnp.int32(n_rep))).wait_recv()

    def e_slot(kind, i, t):
        here = rows_at(i, span)
        if kind == TOK:
            return tok_all.at[t, here]
        if kind == GATED:
            return gated_all.at[t, here]
        return resid_all.at[member if kind == OWN else 1 - member, t, here]

    def x_peer(dx):
        return 2 * flip(xi, dx, n_x) + core

    def e_copy(kind, i, t, k, to):
        slot = e_slot(kind, i, t)
        return copy(slot, slot, e_send.at[kind, i, k], e_recv.at[kind, i, t], tp=to)

    def e_list(kind, i):
        out = [e_copy(kind, i, tp, 0, mate)]
        for dx in range(1, n_x):
            out.append(e_copy(kind, i, tp, dx, x_peer(dx)))
        return out

    def e_push(kind, i):
        for c in e_list(kind, i):
            c.start()

    def e_wait(kind, i, t):
        e_copy(kind, i, t, 0, mate).wait_recv()

    def e_relay(kind, i):
        for dx in range(1, n_x):
            e_wait(kind, i, x_peer(dx))
            e_copy(kind, i, x_peer(dx), n_x - 1 + dx, mate).start()

    def e_finish(kind, i):
        for dx in range(n_x):
            e_wait(kind, i, 2 * flip(xi, dx, n_x) + 1 - core)

    def e_sent(kind, i):
        for c in e_list(kind, i):
            c.wait_send()
        for dx in range(1, n_x):
            e_copy(kind, i, x_peer(dx), n_x - 1 + dx, mate).wait_send()

    def p_copy(i, which):
        slot = resid_all.at[which, tp, rows_at(i, span)]
        return copy(slot, slot, p_send.at[i], p_recv.at[i], fs=pair)

    def o_copy(k, sub):
        to = lax.rem(tp + k, jnp.int32(n_tp))
        return copy(out_gather.at[to * per_own + sub], out_all.at[tp, sub], o_send.at[k - 1, sub],
                    o_recv.at[k - 1, sub], tp=to)

    def o_take(k, sub):
        sender = lax.rem(tp - k + n_tp, jnp.int32(n_tp))
        copy(out_gather.at[0], out_all.at[sender, sub], o_send.at[k - 1, sub], o_recv.at[k - 1, sub],
             tp=mate).wait_recv()

    def o_each(action):
        for k in range(1, n_tp):
            for sub in range(per_own):
                action(k, sub)

    def s_copy(d, which):
        g = flip(fs, d, n_fs)
        src = (out_scale_ref, down_scale_ref)[which]
        return copy(src, scale_all.at[which, owner_sub], s_send.at[which, d - 1], s_recv.at[which, owner_sub], fs=g)

    loads = [
        pltpu.make_async_copy(src, dst, local_sem.at[i])
        for i, (src, dst) in enumerate((
            (tokens_ref, tok_all.at[tp]), (u_ref, u_f), (v_ref, v_f), (out_ref, out_f), (gate_ref, gate_f),
            (up_ref, up_f), (down_ref, down_f)))
    ]
    for load in loads:
        load.start()

    barrier = pltpu.get_barrier_semaphore()

    def greet(**device):
        pl.semaphore_signal(barrier, inc=1, device_id=device, device_id_type=MESH)

    for k in range(1, n_tp):
        greet(tp=lax.rem(tp + k, jnp.int32(n_tp)))
    loop(1, n_fs, lambda d: greet(fs=flip(fs, d, n_fs)))
    for e in range(1, n_rep):
        greet(rep=lax.rem(rep + e, jnp.int32(n_rep)))
    pl.semaphore_wait(barrier, n_tp + n_fs + n_rep - 3)

    loads[0].wait()
    loop(0, spans, lambda i: e_push(TOK, i))
    loads[1].wait()
    loads[2].wait()
    uv_all[fs, :, 0:channels] = u_f[...].astype(jnp.bfloat16)
    uv_all[fs, :, channels:2 * channels] = v_f[...].astype(jnp.bfloat16)
    z_start(UV)
    loads[3].wait()
    out_gather[fs] = out_f[...].astype(jnp.bfloat16)
    z_start(OUT)

    def keep_own():
        scale_all[0, owner_sub] = out_scale_ref[...]
        scale_all[1, owner_sub] = down_scale_ref[...]

    on(owner == tp, keep_own)

    def s_each(action):
        def body(d):
            for which in range(2):
                action(s_copy(d, which))

        on(owner == tp, lambda: loop(1, n_fs, body))

    s_each(lambda c: c.start())

    low = lax.broadcasted_iota(jnp.int32, (1, LANES), 1) < LANES // 2
    unit = 64

    def swap(value):
        return pltpu.roll(value, LANES // 2, 1)

    loads[4].wait()
    loads[5].wait()

    def cast_gu(i):
        here = rows_at(i, unit)
        for member_of in range(2):
            first = member_of * (main + LANES)
            gu_own[member_of, here, 0:main] = gate_f[here, first:first + main].astype(jnp.bfloat16)
            gu_own[member_of, here, main:2 * main] = up_f[here, first:first + main].astype(jnp.bfloat16)
        g, u = gate_f[here, main:main + LANES], up_f[here, main:main + LANES]
        gu_own[0, here, 2 * main:] = jnp.where(low, g, swap(u)).astype(jnp.bfloat16)
        gu_own[1, here, 2 * main:] = jnp.where(low, swap(g), u).astype(jnp.bfloat16)

    loop(0, block // unit, cast_gu)
    z_start(GU, 0, 1)
    keep_gu = pltpu.make_async_copy(gu_own.at[member], gu_all.at[fs], local_sem.at[7])
    keep_gu.start()
    loads[6].wait()

    def cast_down(i):
        here = rows_at(i, unit)
        there = rows_at(jnp.where(i < main // unit, i + (main + LANES) // unit, main // unit + 1), unit)
        for p in range(pieces):
            cols = slice(p * width_down, (p + 1) * width_down)
            down_own[0, p, here] = down_f[here, cols].astype(jnp.bfloat16)
            down_own[1, p, here] = down_f[there, cols].astype(jnp.bfloat16)

    loop(0, hid // unit, cast_down)
    keep_down = pltpu.make_async_copy(down_own.at[member], down_all.at[pl.ds(fs * pieces, pieces)], local_sem.at[8])
    keep_down.start()


    def first_relays(i):
        e_relay(TOK, i)
        on(i + 1 < n_fs, lambda: y_relay(UV, i + 1))

    loop(0, spans, first_relays)
    loop(spans + 1, n_fs, lambda d: y_relay(UV, d))
    loop(1, n_fs, lambda d: y_relay(OUT, d))
    for p in range(1, early_cuts):
        z_start(GU, p, p + 1)
    loop(1, n_fs, lambda d: y_ready(UV, d))

    eye = lax.broadcasted_iota(jnp.int32, (span, span), 0) == lax.broadcasted_iota(jnp.int32, (span, span), 1)
    tril = lax.broadcasted_iota(jnp.int32, (span, span), 0) >= lax.broadcasted_iota(jnp.int32, (span, span), 1)

    def mixer_span(i):
        e_finish(TOK, i)
        here = rows_at(i, span)
        square = jnp.zeros((span, 1), jnp.float32)
        for t in range(n_tp):
            wide = tok_all[t, here, :].astype(jnp.float32)
            square += jnp.sum(wide * wide, axis=-1, keepdims=True)
        inverse = lax.rsqrt(square / (n_tp * own_width) + EPS)
        pre = None
        for f in range(n_fs):
            t, sub = f // per_own, f % per_own
            wide = tok_all[t, here, sub * block:(sub + 1) * block].astype(jnp.float32)
            source = (wide * inverse * pre_gain_ref[:, f * block:(f + 1) * block]).astype(jnp.bfloat16)
            term = jnp.dot(source, uv_all[f], preferred_element_type=jnp.float32)
            pre = term if f == 0 else pre + term
        u_act = jax.nn.gelu(pre[:, :channels] * u_scale_ref[...])
        v_act = jax.nn.gelu(pre[:, channels:] * v_scale_ref[...])
        width = channels // groups
        group_of = lax.broadcasted_iota(jnp.int32, v_act.shape, 1) // width
        centre = jnp.zeros_like(v_act)
        for g in range(groups):
            mean = jnp.sum(jnp.where(group_of == g, v_act, 0.0), axis=-1, keepdims=True) / width
            centre = jnp.where(group_of == g, mean, centre)
        apart = v_act - centre
        square = apart * apart
        inverse = jnp.zeros_like(v_act)
        for g in range(groups):
            spread = jnp.sum(jnp.where(group_of == g, square, 0.0), axis=-1, keepdims=True) / width
            inverse = jnp.where(group_of == g, lax.rsqrt(spread + EPS), inverse)
        v_norm = (apart * inverse * group_gain_ref[...]).astype(jnp.bfloat16)
        mixed = jnp.zeros_like(v_act)
        for g in range(groups):
            lower = jnp.where(tril, span_ref[g].astype(jnp.float32), 0.0).astype(jnp.bfloat16)
            bias = jnp.sum(jnp.where(eye, bias_ref[g:g + 1, :], 0.0), axis=1, keepdims=True)
            term = jnp.dot(lower, v_norm, preferred_element_type=jnp.float32) + bias
            mixed = jnp.where(group_of == g, term, mixed)
        gated_all[tp, here, :] = (u_act * mixed).astype(jnp.bfloat16)
        e_push(GATED, i)

    loop(0, spans, mixer_span)
    loop(1, n_fs, lambda d: y_ready(OUT, d))
    o_each(lambda k, sub: o_copy(k, sub).start())
    for sub in range(per_own):
        out_all[tp, sub] = out_gather[tp * per_own + sub]
    loop(0, spans, lambda i: e_relay(GATED, i))

    def relay_gu(p):
        loop(1, n_fs, lambda d: y_relay(GU, d, p))

    relay_gu(0)

    o_each(o_take)

    def scale_arrived(sub):
        def take():
            for which in range(2):
                copy(out_scale_ref, scale_all.at[which, sub], s_send.at[which, 0], s_recv.at[which, sub],
                     fs=pair).wait_recv()

        on(tp * per_own + sub != fs, take)

    loop(0, per_own, scale_arrived)

    def resid_span(i):
        e_finish(GATED, i)
        here = rows_at(i, span)
        for sub in range(per_own):
            mix = None
            for s in range(n_tp):
                term = jnp.dot(gated_all[s, here, :], out_all[s, sub], preferred_element_type=jnp.float32)
                mix = term if s == 0 else mix + term
            mix = (mix * scale_all[0, sub]).astype(jnp.bfloat16)
            cols = slice(sub * block, (sub + 1) * block)
            resid_all[member, tp, here, cols] = (
                tok_all[tp, here, cols].astype(jnp.float32) + mix.astype(jnp.float32)).astype(jnp.bfloat16)
        e_push(OWN, i)
        p_copy(i, member).start()

    loop(0, spans, resid_span)
    for p in range(early_cuts, cuts):
        z_start(GU, p, p + 1)

    def norm_span(which, i):
        here = rows_at(i, span)
        square = jnp.zeros((span, 1), jnp.float32)
        for t in range(n_tp):
            wide = resid_all[which, t, here, :].astype(jnp.float32)
            square += jnp.sum(wide * wide, axis=-1, keepdims=True)
        inverse = lax.rsqrt(square / (n_tp * own_width) + EPS)
        there = rows_at(which * spans + i, span)
        for f in range(n_fs):
            t, sub = f // per_own, f % per_own
            wide = resid_all[which, t, here, sub * block:(sub + 1) * block].astype(jnp.float32)
            gain = ffn_gain_ref[:, f * block:(f + 1) * block]
            normed[f, there, :] = (wide * inverse * gain).astype(jnp.bfloat16)

    done = 1
    for i in range(spans):
        e_relay(OWN, i)
        if done < early_cuts:
            relay_gu(done)
            done += 1

    def own_span(i):
        e_finish(OWN, i)
        norm_span(member, i)

    loop(0, spans, own_span)
    for p in range(done, early_cuts):
        relay_gu(p)

    outer = jnp.logical_or(fs == 0, fs == n_fs - 1)
    late = max(cuts - 2, early_cuts)

    def relay_one(p, low, high):
        loop(low, high, lambda d: y_relay(GU, d, p))

    on(outer, lambda: relay_one(early_cuts, 2, 3))

    def pair_span(i):
        p_copy(i, 1 - member).wait_recv()
        e_push(PAIR, i)

    loop(0, spans, pair_span)

    def outer_rest():
        for p in range(early_cuts, late):
            relay_one(p, 3 if p == early_cuts else 2, n_fs)
            relay_one(p, 1, 2)

    def inner_rest():
        for p in range(early_cuts, late):
            relay_one(p, 1, n_fs)

    on(outer, outer_rest)
    on(jnp.logical_not(outer), inner_rest)
    loop(0, spans // 2, lambda i: e_relay(PAIR, i))
    for p in range(late, cuts - 1):
        relay_gu(p)
    loop(spans // 2, spans, lambda i: e_relay(PAIR, i))

    def other_span(i):
        e_finish(PAIR, i)
        norm_span(1 - member, i)

    loop(0, spans, other_span)

    keep_gu.wait()

    loop(pieces, units, lambda k: z_copy(DN, *unit_at(k)).start())

    relay_gu(cuts - 1)

    def first_gu(i):
        here = rows_at(i, CHUNK)
        gu_acc[here, :] = jnp.dot(normed[fs, here, :], gu_all[fs], preferred_element_type=jnp.float32)

    loop(0, chunks, first_gu)


    def fold_gu(d):
        for p in range(cuts):
            y_ready(GU, d, p)
        f = flip(fs, d, n_fs)

        def body(i):
            here = rows_at(i, CHUNK)
            gu_acc[here, :] += jnp.dot(normed[f, here, :], gu_all[f], preferred_element_type=jnp.float32)

        loop(0, chunks, body)

    loop(1, n_fs - 1, fold_gu)
    loop(pieces, pieces + 1, lambda k: y_relay(DN, *unit_at(k)))
    fold_gu(jnp.int32(n_fs - 1))

    second = member == 1

    def hidden_chunk(i):
        here = rows_at(i, 64)
        tiles = main // LANES
        for j in range(tiles):
            gate_scale = jnp.where(second, gate_scale_ref[tiles + 1 + j:tiles + 2 + j], gate_scale_ref[j:j + 1])
            up_scale = jnp.where(second, up_scale_ref[tiles + 1 + j:tiles + 2 + j], up_scale_ref[j:j + 1])
            a = gu_acc[here, j * LANES:(j + 1) * LANES] * gate_scale
            b = gu_acc[here, main + j * LANES:main + (j + 1) * LANES] * up_scale
            hidden[here, j * LANES:(j + 1) * LANES] = (a / (1.0 + jnp.exp(-a)) * b).astype(jnp.bfloat16)
        gs, us = gate_scale_ref[tiles:tiles + 1], up_scale_ref[tiles:tiles + 1]
        a = gu_acc[here, 2 * main:] * jnp.where(second, jnp.where(low, swap(gs), us), jnp.where(low, gs, swap(us)))
        b = swap(a)
        last = (a / (1.0 + jnp.exp(-a)) * b).astype(jnp.bfloat16)
        hidden[here, main:hid] = last[:, 0:hid - main]

    loop(0, total_rows // 64, hidden_chunk)
    keep_down.wait()
    loop(pieces + 1, 2 * pieces + 1, lambda k: y_relay(DN, *unit_at(k)))

    def places(s):
        d, p = unit_at(s)
        b = flip(fs, d, n_fs)
        own = lax.div(b, jnp.int32(per_own))
        sub = lax.rem(b, jnp.int32(per_own)) * pieces + p
        return b * pieces + p, lax.rem(own, two), lax.div(own, two), sub, own

    def m_copy(k, j):
        b, oc, ox, sub, own = places(k)
        here = rows_at(j, CHUNK)
        return copy(part.at[b, here], mate_in.at[ox, sub, here], m_send.at[b, j], m_recv.at[ox, sub, j], tp=mate)

    def x_copy(k, j):
        b, oc, ox, sub, own = places(k)
        here = rows_at(j, CHUNK)
        d = flip(xi, ox, n_x)
        return copy(part.at[b, here], x_in.at[d - 1, sub, here], x_send.at[b, j], x_recv.at[d - 1, sub, j], tp=own)

    def q_copy(k, j):
        b, oc, ox, sub, own = places(k)
        src = part.at[b, rows_at((1 - member) * half_chunks + j, CHUNK)]
        return copy(src, pair_in.at[sub, rows_at(j, CHUNK)], q_send.at[sub, j], q_recv.at[sub, j], fs=pair)

    def turned(i):
        return lax.rem((1 - member) * half_chunks + i, jnp.int32(chunks))

    def down_one(k):
        b, oc, ox, sub, own = places(k)
        d, p = unit_at(k)
        on(d > 0, lambda: y_ready(DN, d, p))

        def body(i):
            j = turned(i)
            here = rows_at(j, CHUNK)
            part[b, here, :] = jnp.dot(hidden[here, :], down_all[b], preferred_element_type=jnp.float32).astype(
                jnp.bfloat16)
            on(core != oc, lambda: m_copy(k, j).start())

        loop(0, chunks, body)

    def across(k):
        b, oc, ox, sub, own = places(k)

        def body(i):
            j = turned(i)
            here = rows_at(j, CHUNK)
            m_copy(k, j).wait_recv()
            part[b, here, :] = (part[b, here, :].astype(jnp.float32)
                                + mate_in[ox, sub, here, :].astype(jnp.float32)).astype(jnp.bfloat16)
            on(xi != ox, lambda: x_copy(k, j).start())

        on(core == oc, lambda: loop(0, chunks, body))

    def collect(k):
        b, oc, ox, sub, own = places(k)

        def body(jj):
            j = turned(jj)
            here = rows_at(j, CHUNK)
            total = part[b, here, :].astype(jnp.float32)
            for dx in range(1, n_x):
                copy(part.at[b, here], x_in.at[dx - 1, sub, here], x_send.at[b, j], x_recv.at[dx - 1, sub, j],
                     tp=mate).wait_recv()
                total += x_in[dx - 1, sub, here, :].astype(jnp.float32)
            part[b, here, :] = total.astype(jnp.bfloat16)
            on(jj < half_chunks, lambda: q_copy(k, jj).start())

        on(own == tp, lambda: loop(0, chunks, body))

    def down_step(step):
        down_one(step)
        across(step)
        on(jnp.logical_and(step >= 2 * pieces - 1, step + 2 < units), lambda: y_relay(DN, *unit_at(step + 2)))

    loop(0, units, down_step)
    loop(0, units, collect)

    for sub in range(per_owner):
        b = tp * per_owner + sub
        cols = slice(sub * width_down, (sub + 1) * width_down)

        def close(j, b=b, sub=sub, cols=cols):
            here = rows_at(j, CHUNK)
            copy(part.at[b, here], pair_in.at[sub, here], q_send.at[sub, j], q_recv.at[sub, j], fs=pair).wait_recv()
            mine = rows_at(member * half_chunks + j, CHUNK)
            total = part[b, mine, :].astype(jnp.float32) + pair_in[sub, here, :].astype(jnp.float32)
            total = (total * scale_all[1, sub // pieces, :, sub % pieces * width_down:(sub % pieces + 1) * width_down]).astype(jnp.bfloat16).astype(jnp.float32)
            kept = resid_all[member, tp, here, cols].astype(jnp.float32)
            result_ref[here, cols] = (kept + total).astype(jnp.bfloat16)

        loop(0, half_chunks, close)

    for kind, count in ((UV, 1), (OUT, 1), (GU, cuts), (DN, pieces)):
        def sent(d, kind=kind, count=count):
            for p in range(count):
                if kind in (UV, OUT):
                    on(d == 3, lambda: z_pass(kind).wait_send())
                    on(d != 3, lambda: z_copy(kind, d, p).wait_send())
                else:
                    z_copy(kind, d, p).wait_send()
                for e in range(1, n_rep):
                    y_copy(kind, d, e, p).wait_send()

        loop(1, n_fs, sent)

    def spans_sent(i):
        for kind in range(4):
            e_sent(kind, i)
        p_copy(i, member).wait_send()

    loop(0, spans, spans_sent)
    o_each(lambda k, sub: o_copy(k, sub).wait_send())
    s_each(lambda c: c.wait_send())

    def parts_sent(k):
        b, oc, ox, sub, own = places(k)

        def body(j):
            on(core != oc, lambda: m_copy(k, j).wait_send())
            on(jnp.logical_and(core == oc, xi != ox), lambda: x_copy(k, j).wait_send())
            on(jnp.logical_and(own == tp, j < half_chunks), lambda: q_copy(k, j).wait_send())

        loop(0, chunks, body)

    loop(0, units, parts_sent)


def shards(
    sizes,
    tokens,
    pre_gain,
    u_weight,
    u_scale,
    v_weight,
    v_scale,
    group_gain,
    span_weight,
    span_bias,
    out_weight,
    out_scale,
    ffn_gain,
    gate_weight,
    gate_scale,
    up_weight,
    up_scale,
    down_weight,
    down_scale,
):
    n_rep, n_fs, n_tp = sizes
    n_x = n_tp // 2
    extra = (LANES - gate_weight.shape[1]) % (2 * LANES)
    if extra:
        gate_weight, up_weight = (jnp.pad(w, ((0, 0), (0, extra))) for w in (gate_weight, up_weight))
        gate_scale, up_scale = (jnp.pad(s, (0, extra)) for s in (gate_scale, up_scale))
        down_weight = jnp.pad(down_weight, ((0, extra), (0, 0)))
    rows, own_width = tokens.shape
    block, local_hidden = gate_weight.shape
    hid = local_hidden // 2
    channels = u_weight.shape[1]
    per_own = own_width // block
    spans = rows // span_weight.shape[1]
    chunks = 2 * rows // CHUNK
    pieces = max(block // (2 * LANES), 1)
    width_down, per_owner, units = block // pieces, per_own * pieces, n_fs * pieces
    row = lambda vector: vector.reshape(1, -1)
    operands = (
        tokens, u_weight, v_weight, out_weight, gate_weight, up_weight, down_weight, row(out_scale), row(down_scale),
        row(pre_gain), row(ffn_gain), row(u_scale), row(v_scale), row(group_gain), span_weight, span_bias,
        gate_scale.reshape(-1, LANES), up_scale.reshape(-1, LANES),
    )
    hbm, vmem = pl.BlockSpec(memory_space=pl.ANY), pl.BlockSpec(memory_space=pltpu.VMEM)
    bf16, f32 = jnp.bfloat16, jnp.float32
    dma = lambda *shape: pltpu.SemaphoreType.DMA(shape)
    return pl.pallas_call(
        functools.partial(layer_kernel, sizes),
        out_shape=jax.ShapeDtypeStruct((rows, own_width), bf16),
        in_specs=[hbm] * 7 + [vmem] * 11,
        out_specs=vmem,
        scratch_shapes=[
            pltpu.VMEM((block, channels), f32),
            pltpu.VMEM((block, channels), f32),
            pltpu.VMEM((channels, block), f32),
            pltpu.VMEM((block, local_hidden), f32),
            pltpu.VMEM((block, local_hidden), f32),
            pltpu.VMEM((local_hidden, block), f32),
            pltpu.VMEM((2, block, 2 * hid), bf16),
            pltpu.VMEM((2, pieces, hid, width_down), bf16),
            pltpu.VMEM((n_tp, rows, own_width), bf16),
            pltpu.VMEM((n_fs, block, 2 * channels), bf16),
            pltpu.VMEM((n_fs, channels, block), bf16),
            pltpu.VMEM((n_tp, per_own, channels, block), bf16),
            pltpu.VMEM((2, per_own, 1, block), f32),
            pltpu.VMEM((n_tp, rows, channels), bf16),
            pltpu.VMEM((2, n_tp, rows, own_width), bf16),
            pltpu.VMEM((n_fs, 2 * rows, block), bf16),
            pltpu.VMEM((n_fs, block, 2 * hid), bf16),
            pltpu.VMEM((units, hid, width_down), bf16),
            pltpu.VMEM((2 * rows, 2 * hid), f32),
            pltpu.VMEM((2 * rows, hid), bf16),
            pltpu.VMEM((units, 2 * rows, width_down), bf16),
            pltpu.VMEM((n_x, per_owner, 2 * rows, width_down), bf16),
            pltpu.VMEM((n_x - 1, per_owner, 2 * rows, width_down), bf16),
            pltpu.VMEM((per_owner, rows, width_down), bf16),
            dma(9),
            dma(DN + pieces, n_fs - 1),
            dma(DN + pieces, n_fs - 1),
            dma(DN + pieces, n_fs - 1, n_rep - 1),
            dma(DN + pieces, n_fs - 1, n_rep - 1),
            dma(4, spans, n_tp - 1),
            dma(4, spans, n_tp),
            dma(spans),
            dma(spans),
            dma(n_tp - 1, per_own),
            dma(n_tp - 1, per_own),
            dma(2, n_fs - 1),
            dma(2, per_own),
            dma(units, chunks),
            dma(n_x, per_owner, chunks),
            dma(units, chunks),
            dma(n_x - 1, per_owner, chunks),
            dma(per_owner, chunks // 2),
            dma(per_owner, chunks // 2),
        ],
        compiler_params=pltpu.CompilerParams(
            collective_id=0, has_side_effects=True, vmem_limit_bytes=63 * 1024 * 1024
        ),
    )(*operands)


def solution(mesh):
    placed = (
        P(("rep", "fs"), "tp"),
        P(),
        P("fs", "tp"),
        P("tp"),
        P("fs", "tp"),
        P("tp"),
        P("tp"),
        P("tp", None, None),
        P("tp", None),
        P("tp", "fs"),
        P("fs"),
        P(),
        P("fs", "tp"),
        P("tp"),
        P("fs", "tp"),
        P("tp"),
        P("tp", "fs"),
        P("fs"),
    )
    sizes = (mesh.shape["rep"], mesh.shape["fs"], mesh.shape["tp"])
    return jax.shard_map(
        functools.partial(shards, sizes), mesh=mesh, in_specs=placed, out_specs=P(("rep", "fs"), "tp"), check_vma=False
    )
```
